128 devices in a mesh: ep: 32 (over z, y, core), tp: 4 (over x).
Axes of the slice: x: 4, y: 4, z: 4, core: 2. Of those that a mesh axis runs over, the one named last changes fastest.
Arguments:
- gate_outer: bfloat16 [65536, 1024], P(('ep', 'tp')), may hold values from -6 to 6
- gate_inner: bfloat16 [65536, 1024], P(('ep', 'tp')), may hold values from -6 to 6
- conv_input: bfloat16 [65536, 1024], P(('ep', 'tp')), may hold values from -6 to 6
- conv_taps: float32 [3, 1024], replicated, may hold values from -3.5 to 3.5
- mixer_out_weight: bfloat16 [1024, 2048], replicated, may hold values from -0.1875 to 0.1875
- moe_tokens: bfloat16 [16384, 2048], P(('ep', 'tp')), may hold values from -40 to 40
- norm_gain: float32 [2048], replicated, may hold values from 0.1 to 1.9
- expert_ids: int32 [16384, 4], P(('ep', 'tp')), may hold values from 0 to 127, all different within a row; in each aligned block of 128 rows (0 to 127, 128 to 255, ...) at most 6 rows name the same one
- route_weight: float32 [16384, 4], P(('ep', 'tp')), may hold values from 0.2 to 1
- expert_gate: bfloat16 [128, 2048, 1024], P(('ep', 'tp')), may hold values from -0.39648438 to 0.39648438
- expert_up: bfloat16 [128, 2048, 1024], P(('ep', 'tp')), may hold values from -0.39648438 to 0.39648438
- expert_down: bfloat16 [128, 1024, 2048], P(('ep', 'tp')), may hold values from -0.03125 to 0.03125
Outputs:
- mixed_out: bfloat16 [65536, 2048], P(('ep', 'tp'))
- moe_out: bfloat16 [16384, 2048], P(('ep', 'tp'))
The draws below stay inside these ranges and needn't reach their ends.
Inputs may be any that keep to these rules, and one draw needn't show every extreme that they name: `expert_ids`: each token names 4 different experts. Among the tokens of one device no expert is named by more than 6 of them, and on some device an expert is named by exactly 6.
All inputs are finite; a program needn't handle non-finite values.
Results may differ from the reference program's by a relative error of at most 0.007.
Values may be sent and summed in bfloat16 or wider, within the bound.
A program may use at most 128 MiB of HBM per device.

```python
import math
import jax
import jax.numpy as jnp
import numpy as np
from jax import lax

D = 2048
W_MIX = 1024
FF = 1024
TOP_K = 4
TAPS = 3
MOE_DEV = 128
EXPERTS = 128
CAP = 6
MIX_TOKENS = 65536
MOE_TOKENS = 16384
DEVICES = 128


def draw_moe_tokens(key, part):
    key_base = jax.random.fold_in(key, 101)
    key_scale = jax.random.fold_in(key, 202)
    base_values = jax.random.truncated_normal(key_base, -4.0, 4.0, (MOE_TOKENS, D), jnp.float32)
    row_scale = jnp.exp(jax.random.uniform(key_scale, (MOE_TOKENS, 1), jnp.float32, 0.0, math.log(10.0)))
    values = base_values * row_scale
    return values.astype(jnp.bfloat16)


def level_of(stream_key, extent, cuts, low, top_value):
    def one(axis_at, parts):
        heights = jax.random.uniform(jax.random.fold_in(jax.random.fold_in(stream_key, 6), axis_at), (parts,), jnp.float32, low / len(cuts), top_value / len(cuts))
        return jnp.repeat(jnp.exp(heights), extent[axis_at] // parts).reshape((-1,) + (1,) * (len(extent) - axis_at - 1))

    loudness = one(*cuts[0])
    for cut in cuts[1:]:
        loudness = loudness * one(*cut)
    return loudness


def shared_out(rng, own, number, rows, amount, top, reach, slope):
    ranking = jax.random.permutation(rng, amount)
    crowded, usual = shares(amount, rows * top, reach, slope, True), shares(amount, rows * top, reach, slope, False)
    places = jnp.arange(amount)

    def named(sizes, turn):
        used = int((sizes > 0).sum())
        fixed = max(1, used // 4)
        passed = fixed + (places - fixed + turn * (used - fixed)) % max(1, amount - fixed)
        return jnp.zeros((amount,), jnp.int32).at[ranking[jnp.where(places < fixed, places, passed)]].set(jnp.asarray(sizes, jnp.int32))

    sizes = jnp.where(number % 4 == 0, named(crowded, number // 4), named(usual, number - number // 4 - 1))
    mixed = jax.random.permutation(jax.random.fold_in(own, 3), amount)
    donor, receiver = mixed[0:amount // 2 * 2:2], mixed[1:amount // 2 * 2:2]
    room = jnp.minimum(sizes[donor] - 1, reach - sizes[receiver]) // 2
    room = jnp.where((donor == ranking[0]) | (receiver == ranking[0]) | (sizes[receiver] == 0), 0, jnp.maximum(room, 0))
    passed = jax.random.randint(jax.random.fold_in(own, 4), (amount // 2,), 0, 1 << 20) % (room + 1)
    sizes = sizes.at[donor].add(-passed).at[receiver].add(passed)
    labels = jnp.searchsorted(jnp.cumsum(sizes), jnp.arange(rows * top), side="right").astype(jnp.int32)
    listing = labels.reshape(top, rows).T
    listing = listing[jax.random.permutation(jax.random.fold_in(own, 1), rows)]
    turn = jax.random.randint(jax.random.fold_in(own, 2), (rows, 1), 0, top)
    return jnp.take_along_axis(listing, (jnp.arange(top)[None, :] + turn) % top, axis=1)


def shares(count, total, reach, skew, full):
    portions = [(1 << 20) // math.isqrt(grade ** skew) + 1 for grade in range(1, count + 1)]
    largest = reach if full else min(reach, max(-(-total // count), total * portions[0] // sum(portions)))
    least = 1 if total - largest >= count - 1 else 0
    given, spare = [largest] + [least] * (count - 1), total - largest - least * (count - 1)
    while spare > 0:
        free = [i for i in range(1, count) if given[i] < largest] or [i for i in range(1, count) if given[i] < reach]
        pool, left = sum([portions[i] for i in free]), spare
        for i in free:
            extra = min(reach - given[i], max(1, left * portions[i] // pool), spare)
            given[i] = given[i] + extra
            spare = spare - extra
    return np.array(given)


def scatter_about(key, shape, scale, most, cuts=(), kind=jnp.bfloat16):
    entries = jax.random.normal(key, shape, jnp.float32) * scale
    if len(cuts) > 0:
        entries = level_of(key, shape, cuts, -0.22, 0.18) * entries
    return jnp.clip(entries, min=-most, max=most).astype(kind)


def setup_inputs(seed: int = 0) -> dict:
    splits = jax.random.split(jax.random.key(seed), 13)
    gate_outer = scatter_about(splits[0], (MIX_TOKENS, W_MIX), 1.0, 6.0, ((0, 128),))
    gate_inner = scatter_about(splits[1], (MIX_TOKENS, W_MIX), 1.0, 6.0, ((0, 128),))
    conv_input = scatter_about(splits[2], (MIX_TOKENS, W_MIX), 1.0, 6.0, ((0, 128),))
    conv_taps = scatter_about(splits[3], (TAPS, W_MIX), TAPS ** -0.5, 3.5, (), jnp.float32)
    mixer_out_weight = scatter_about(splits[4], (W_MIX, D), W_MIX ** -0.5, 0.1875)
    moe_tokens = draw_moe_tokens(jax.random.fold_in(splits[12], 71), 0)
    norm_gain = jnp.clip(1.0 + 0.18 * jax.random.normal(splits[6], (D,), jnp.float32), 0.1, 1.9)
    expert_ids_keys = jax.random.split(jax.random.fold_in(splits[7], 1), MOE_TOKENS // MOE_DEV)
    expert_ids_turns = jax.random.permutation(jax.random.fold_in(splits[7], 3), MOE_TOKENS // MOE_DEV)
    expert_ids = jax.vmap(lambda own, number: shared_out(jax.random.fold_in(splits[7], 2), own, number, MOE_DEV, EXPERTS, TOP_K, CAP, 2))(expert_ids_keys, expert_ids_turns).reshape((MOE_TOKENS, TOP_K))
    route_weight = jnp.clip(jnp.exp(math.log(1.0) - 1.609438 * jax.random.uniform(splits[8], (MOE_TOKENS, TOP_K), jnp.float32) ** level_of(splits[8], (MOE_TOKENS, TOP_K), ((0, 128),), -0.2, 0.2)), 0.2, 1.0)
    expert_gate = scatter_about(splits[9], (EXPERTS, D, FF), (3.0 * D ** -0.5), 0.39648438, ((0, 128),))
    expert_up = scatter_about(splits[10], (EXPERTS, D, FF), (3.0 * D ** -0.5), 0.39648438, ((0, 128),))
    expert_down = scatter_about(splits[11], (EXPERTS, FF, D), (FF ** -0.5 / 6.0), 0.03125, ((0, 128),))
    return {"gate_outer": gate_outer, "gate_inner": gate_inner, "conv_input": conv_input, "conv_taps": conv_taps, "mixer_out_weight": mixer_out_weight, "moe_tokens": moe_tokens, "norm_gain": norm_gain, "expert_ids": expert_ids, "route_weight": route_weight, "expert_gate": expert_gate, "expert_up": expert_up, "expert_down": expert_down}


epsilon = 1e-06
clamp_limit = 7.0
alpha_gate = 1.702

def expert_rows(row_block, gate_weight, up_weight, down_weight):
    gate_pre = jnp.dot(row_block, gate_weight, preferred_element_type=jnp.float32)
    up_pre = jnp.dot(row_block, up_weight, preferred_element_type=jnp.float32)
    gate_pre = jnp.minimum(gate_pre, clamp_limit)
    up_pre = jnp.clip(up_pre, -clamp_limit, clamp_limit)
    hidden = ((up_pre + 1.0) * (gate_pre * jax.nn.sigmoid(alpha_gate * gate_pre))).astype(jnp.bfloat16)
    return jnp.dot(hidden, down_weight, preferred_element_type=jnp.float32).astype(jnp.bfloat16)

def reference(gate_outer, gate_inner, conv_input, conv_taps, mixer_out_weight, moe_tokens, norm_gain, expert_ids, route_weight, expert_gate, expert_up, expert_down):
    product = (gate_inner.astype(jnp.float32) * conv_input.astype(jnp.float32)).astype(jnp.bfloat16)
    padded = jnp.concatenate([jnp.zeros((TAPS - 1, W_MIX), jnp.float32), product.astype(jnp.float32)], 0)
    convolved = jnp.zeros((MIX_TOKENS, W_MIX), jnp.float32)
    for offset in range(TAPS):
        convolved = convolved + conv_taps[offset][None, :] * padded[offset:offset + MIX_TOKENS]
    gated = (gate_outer.astype(jnp.float32) * convolved).astype(jnp.bfloat16)
    mixed_out = jnp.dot(gated, mixer_out_weight, preferred_element_type=jnp.float32).astype(jnp.bfloat16)
    widened = moe_tokens.astype(jnp.float32)
    normed = (widened * lax.rsqrt(lax.optimization_barrier(jnp.mean(widened * widened, axis=-1, keepdims=True)) + epsilon) * norm_gain.astype(jnp.float32)).astype(jnp.bfloat16)
    mix_weight = route_weight / lax.optimization_barrier(jnp.sum(route_weight, axis=-1, keepdims=True))
    flat_ids = expert_ids.reshape(-1).astype(jnp.int32)
    copy_weight = mix_weight.reshape(-1)
    copy_order = jnp.argsort(flat_ids, stable=True).astype(jnp.int32)
    counts = jax.ops.segment_sum(jnp.ones_like(flat_ids), flat_ids, EXPERTS).astype(jnp.int32)
    starts = (jnp.cumsum(counts) - counts).astype(jnp.int32)
    row_limit = DEVICES * CAP
    order_padded = jnp.concatenate([copy_order, jnp.zeros((row_limit,), jnp.int32)], 0)
    positions = jnp.arange(row_limit, dtype=jnp.int32)

    def per_expert(totals, expert):
        picked = lax.dynamic_slice_in_dim(order_padded, starts[expert].astype(jnp.int32), row_limit)
        is_valid = positions < counts[expert]
        token_index = (picked // TOP_K).astype(jnp.int32)
        row_block = normed[token_index]
        expert_out = expert_rows(row_block, expert_gate[expert], expert_up[expert], expert_down[expert])
        scaled = jnp.where(is_valid, copy_weight[picked], jnp.zeros_like(copy_weight[picked]))
        totals = totals.at[token_index].add(scaled[:, None] * expert_out.astype(jnp.float32))
        return (totals, None)
    totals, _ = lax.scan(per_expert, jnp.zeros((MOE_TOKENS, D), jnp.float32), jnp.arange(EXPERTS, dtype=jnp.int32))
    moe_out = totals.astype(jnp.bfloat16)
    return (mixed_out, moe_out)
```

```python
import functools

import jax
import jax.numpy as jnp
import numpy as np
from jax import lax
from jax.experimental import pallas as pl
from jax.experimental.pallas import tpu as pltpu
from jax.sharding import PartitionSpec as P

epsilon = 1e-06
clamp_limit = 7.0
alpha_gate = 1.702
MESH = pl.DeviceIdType.MESH

SIDE = 4
CORES = 2


def peer_order():
    def hops(off):
        return sum(min(v, SIDE - v) for v in off[:3])

    offs = [
        (dz, dy, dx, dk)
        for dz in range(SIDE)
        for dy in range(SIDE)
        for dx in range(SIDE)
        for dk in range(CORES)
    ][1:]
    state = 12345
    keyed = []
    for off in offs:
        state = (state * 1103515245 + 12345) % (1 << 31)
        keyed.append((-hops(off), state >> 8, off))
    return [k[2] for k in sorted(keyed)] + [(0, 0, 0, 0)]


ORDER = peer_order()
PEERS = len(ORDER)
GROUP = 8
CHUNK = 16
CHUNKS = PEERS // CHUNK
ROWS = CHUNK * GROUP


def kernel(
    cap,
    go_hbm,
    gi_hbm,
    ci_hbm,
    taps_hbm,
    wmix_hbm,
    tok_hbm,
    gain_hbm,
    ids_hbm,
    rw_hbm,
    offs_hbm,
    wg_hbm,
    wu_hbm,
    wd_hbm,
    mixed_hbm,
    moe_hbm,
    go,
    gi,
    ci,
    taps,
    wmix,
    tok,
    gain,
    ids,
    rw,
    offs,
    wg,
    wu,
    wd,
    mixed,
    moe,
    send,
    recv,
    ret,
    pick,
    comb,
    prod,
    tail,
    halo,
    normed,
    acc,
    lsem,
    osem,
    dsend,
    drecv,
    rsend,
    rrecv,
    hsem,
):
    ep = lax.axis_index("ep")
    tp = lax.axis_index("tp")
    z = ep // (SIDE * CORES)
    y = (ep // CORES) % SIDE
    k = ep % CORES
    x = tp

    def local(i, src, dst):
        copy = pltpu.make_async_copy(src, dst, lsem.at[i])
        copy.start()
        return copy

    small = [
        local(0, tok_hbm, tok),
        local(1, ids_hbm, ids),
        local(2, rw_hbm, rw),
        local(3, gain_hbm, gain),
        local(4, offs_hbm, offs),
    ]

    zs = [(z + d) % SIDE * (SIDE * CORES) for d in range(SIDE)]
    zn = [(z + SIDE - d) % SIDE * (SIDE * CORES) for d in range(SIDE)]
    ys = [(y + d) % SIDE * CORES for d in range(SIDE)]
    yn = [(y + SIDE - d) % SIDE * CORES for d in range(SIDE)]
    xs = [(x + d) % SIDE for d in range(SIDE)]
    xn = [(x + SIDE - d) % SIDE for d in range(SIDE)]
    ks = [(k + d) % CORES for d in range(CORES)]

    def ahead(i):
        dz, dy, dx, dk = ORDER[i]
        return (zs[dz] + ys[dy] + ks[dk], xs[dx])

    def behind(i):
        dz, dy, dx, dk = ORDER[i]
        return (zn[dz] + yn[dy] + ks[dk], xn[dx])

    barrier = pltpu.get_barrier_semaphore()
    for i in range(PEERS - 1):
        pl.semaphore_signal(barrier, inc=1, device_id=ahead(i), device_id_type=MESH)

    mix_in = [
        local(5, gi_hbm, gi),
        local(6, ci_hbm, ci),
        local(7, go_hbm, go),
        local(8, taps_hbm, taps),
        local(9, wmix_hbm, wmix),
    ]
    experts_in = [
        local(10, wg_hbm, wg),
        local(11, wu_hbm, wu),
        local(12, wd_hbm, wd),
    ]

    for copy in small:
        copy.wait()
    wide = tok[...].astype(jnp.float32)
    mean = jnp.mean(wide * wide, axis=-1, keepdims=True)
    normed[...] = (wide * lax.rsqrt(mean + epsilon) * gain[...]).astype(jnp.bfloat16)

    tokens = tok.shape[0]
    off = offs[...]
    oz, oy, ok, ox = off // 32, (off // 8) % SIDE, (off // 4) % CORES, off % SIDE
    target = (
        (z + oz) % SIDE * 32 + (y + oy) % SIDE * 8 + (k + ok) % CORES * 4 + (x + ox) % SIDE
    )
    weights = rw[...]
    weights = weights / jnp.sum(weights, axis=0, keepdims=True)
    named = jnp.zeros((PEERS, tokens), jnp.float32)
    named_weight = jnp.zeros((PEERS, tokens), jnp.float32)
    for j in range(ids.shape[0]):
        hit = ids[j : j + 1, :] == target
        named = jnp.where(hit, 1.0, named)
        named_weight = jnp.where(hit, weights[j : j + 1, :], named_weight)
    earlier = (
        lax.broadcasted_iota(jnp.int32, (tokens, tokens), 0)
        < lax.broadcasted_iota(jnp.int32, (tokens, tokens), 1)
    ).astype(jnp.bfloat16)
    rank = jnp.dot(named.astype(jnp.bfloat16), earlier, preferred_element_type=jnp.float32)
    rank = jnp.where(named > 0.5, rank, 99.0)
    place = lax.broadcasted_iota(jnp.int32, (PEERS, GROUP, tokens), 1).astype(jnp.float32)
    chosen = jnp.broadcast_to(rank[:, None, :], (PEERS, GROUP, tokens)) == place
    pick[...] = (
        jnp.where(chosen, 1.0, 0.0).reshape(PEERS * GROUP, tokens).astype(jnp.bfloat16)
    )

    def dispatch(i):
        rows = pl.ds(i * GROUP, cap)
        return pltpu.make_async_remote_copy(
            send.at[rows],
            recv.at[rows],
            dsend,
            drecv.at[i // CHUNK],
            device_id=ahead(i),
            device_id_type=MESH,
        )

    def giveback(i):
        rows = pl.ds(i * GROUP, cap)
        return pltpu.make_async_remote_copy(
            recv.at[rows],
            ret.at[rows],
            rsend,
            rrecv.at[i // CHUNK],
            device_id=behind(i),
            device_id_type=MESH,
        )

    def peers_of(c):
        return range(c * CHUNK, min((c + 1) * CHUNK, PEERS - 1))

    def all_rows(ref, sem, count):
        part = ref.at[pl.ds(0, count * GROUP), pl.ds(0, ref.shape[1] * cap // GROUP)]
        return pltpu.make_async_copy(part, part, sem)

    for c in range(CHUNKS):
        rows = pl.ds(c * ROWS, ROWS)
        send[rows, :] = jnp.dot(
            pick[rows, :], normed[...], preferred_element_type=jnp.float32
        ).astype(jnp.bfloat16)
        if c == 0:
            pl.semaphore_wait(barrier, PEERS - 1)
        else:
            for i in peers_of(c - 1):
                dispatch(i).start()
    for i in peers_of(CHUNKS - 1):
        dispatch(i).start()
    own = pl.ds((PEERS - 1) * GROUP, GROUP)
    recv[own, :] = send[own, :]

    reach = taps.shape[0] - 1
    positions = gi.shape[0]
    for copy in mix_in[:2]:
        copy.wait()
    last = pl.ds(positions - 16, 16)
    tail[...] = (gi[last, :].astype(jnp.float32) * ci[last, :].astype(jnp.float32)).astype(
        jnp.bfloat16
    )
    here = ep * SIDE + tp
    after = (here + 1) % PEERS
    halo_copy = pltpu.make_async_remote_copy(
        tail.at[pl.ds(8, 8)],
        halo.at[pl.ds(8, 8)],
        hsem.at[0],
        hsem.at[1],
        device_id=(after // SIDE, after % SIDE),
        device_id_type=MESH,
    )
    halo_copy.start()

    block = 128

    @pl.loop(0, positions // block)
    def _(b):
        rows = pl.ds(pl.multiple_of(b * block, block), block)
        prod[pl.ds(pl.multiple_of(8 + b * block, 8), block), :] = (
            (gi[rows, :].astype(jnp.float32) * ci[rows, :].astype(jnp.float32))
            .astype(jnp.bfloat16)
            .astype(jnp.float32)
        )

    for c in range(CHUNKS):
        group = rank[c * CHUNK : (c + 1) * CHUNK]
        group_weight = named_weight[c * CHUNK : (c + 1) * CHUNK]
        shape = (CHUNK, GROUP, tokens)
        share = jnp.where(
            jnp.broadcast_to(group[:, None, :], shape) == place[:CHUNK],
            jnp.broadcast_to(group_weight[:, None, :], shape),
            0.0,
        ).reshape(ROWS, tokens)
        comb[c] = share.T.astype(jnp.bfloat16)

    for copy in mix_in[2:]:
        copy.wait()
    halo_copy.wait()
    prod[0:8, :] = jnp.where(here == 0, 0.0, halo[8:16, :].astype(jnp.float32))

    @pl.loop(0, positions // block)
    def _(b):
        rows = pl.ds(pl.multiple_of(b * block, block), block)
        window = prod[pl.ds(pl.multiple_of(b * block, 8), block + 8), :]
        convolved = jnp.zeros((block, window.shape[1]), jnp.float32)
        for j in range(reach + 1):
            start = 8 - reach + j
            convolved = convolved + taps[j : j + 1, :] * window[start : start + block]
        gated = (go[rows, :].astype(jnp.float32) * convolved).astype(jnp.bfloat16)
        mixed[rows, :] = jnp.dot(
            gated, wmix[...], preferred_element_type=jnp.float32
        ).astype(jnp.bfloat16)

    mixed_copy = pltpu.make_async_copy(mixed, mixed_hbm, osem.at[0])
    mixed_copy.start()

    for copy in experts_in:
        copy.wait()

    @pl.loop(0, CHUNKS)
    def _(c):
        for n in range(CHUNKS):

            @pl.when(c == n)
            def _():
                all_rows(recv, drecv.at[n], len(peers_of(n))).wait()

        rows = pl.ds(pl.multiple_of(c * ROWS, ROWS), ROWS)
        block_rows = recv[rows, :]
        hidden = []
        width = 256
        for n in range(0, wg.shape[1], width):
            gate_pre = jnp.dot(
                block_rows, wg[:, n : n + width], preferred_element_type=jnp.float32
            )
            up_pre = jnp.dot(
                block_rows, wu[:, n : n + width], preferred_element_type=jnp.float32
            )
            gate_pre = jnp.minimum(gate_pre, clamp_limit)
            up_pre = jnp.clip(up_pre, -clamp_limit, clamp_limit)
            hidden.append(
                ((up_pre + 1.0) * (gate_pre * jax.nn.sigmoid(alpha_gate * gate_pre))).astype(
                    jnp.bfloat16
                )
            )
        hidden = jnp.concatenate(hidden, axis=1)
        for n in range(0, wd.shape[1], width):
            recv[rows, n : n + width] = jnp.dot(
                hidden, wd[:, n : n + width], preferred_element_type=jnp.float32
            ).astype(jnp.bfloat16)
        for n in range(CHUNKS):

            @pl.when(c == n)
            def _():
                for i in peers_of(n):
                    giveback(i).start()

    ret[own, :] = recv[own, :]

    acc[...] = jnp.zeros_like(acc)
    used = lax.broadcasted_iota(jnp.int32, (ROWS, ret.shape[1]), 0) % GROUP < cap

    @pl.loop(0, CHUNKS)
    def _(c):
        for n in range(CHUNKS):

            @pl.when(c == n)
            def _():
                all_rows(ret, rrecv.at[n], len(peers_of(n))).wait()

        rows = pl.ds(pl.multiple_of(c * ROWS, ROWS), ROWS)
        back = jnp.where(used, ret[rows, :].astype(jnp.float32), 0.0).astype(jnp.bfloat16)
        acc[...] += jnp.dot(comb[c], back, preferred_element_type=jnp.float32)

    moe[...] = acc[...].astype(jnp.bfloat16)
    moe_copy = pltpu.make_async_copy(moe, moe_hbm, osem.at[1])
    moe_copy.start()
    all_rows(send, dsend, PEERS - 1).wait()
    all_rows(recv, rsend, PEERS - 1).wait()
    mixed_copy.wait()
    moe_copy.wait()


def shards(
    gate_outer,
    gate_inner,
    conv_input,
    conv_taps,
    mixer_out_weight,
    moe_tokens,
    norm_gain,
    expert_ids,
    route_weight,
    expert_gate,
    expert_up,
    expert_down,
):
    positions, channels = gate_inner.shape
    tokens, width = moe_tokens.shape
    hidden = expert_gate.shape[2]
    choices = expert_ids.shape[1]
    cap = 3 * tokens * choices // (2 * PEERS)
    offsets = np.array([dz * 32 + dy * 8 + dk * 4 + dx for dz, dy, dx, dk in ORDER], np.int32)
    offsets = jnp.asarray(np.broadcast_to(offsets[:, None], (PEERS, tokens)))
    bf16, f32 = jnp.bfloat16, jnp.float32
    anywhere = pl.BlockSpec(memory_space=pl.ANY)
    slots = (PEERS * GROUP, width)
    return pl.pallas_call(
        functools.partial(kernel, cap),
        out_shape=(
            jax.ShapeDtypeStruct((positions, width), bf16),
            jax.ShapeDtypeStruct((tokens, width), bf16),
        ),
        in_specs=[anywhere] * 13,
        out_specs=(anywhere, anywhere),
        scratch_shapes=[
            pltpu.VMEM((positions, channels), bf16),
            pltpu.VMEM((positions, channels), bf16),
            pltpu.VMEM((positions, channels), bf16),
            pltpu.VMEM(conv_taps.shape, f32),
            pltpu.VMEM((channels, width), bf16),
            pltpu.VMEM((tokens, width), bf16),
            pltpu.VMEM((1, width), f32),
            pltpu.VMEM((choices, tokens), jnp.int32),
            pltpu.VMEM((choices, tokens), f32),
            pltpu.VMEM((PEERS, tokens), jnp.int32),
            pltpu.VMEM((width, hidden), bf16),
            pltpu.VMEM((width, hidden), bf16),
            pltpu.VMEM((hidden, width), bf16),
            pltpu.VMEM((positions, width), bf16),
            pltpu.VMEM((tokens, width), bf16),
            pltpu.VMEM(slots, bf16),
            pltpu.VMEM(slots, bf16),
            pltpu.VMEM(slots, bf16),
            pltpu.VMEM((PEERS * GROUP, tokens), bf16),
            pltpu.VMEM((CHUNKS, tokens, ROWS), bf16),
            pltpu.VMEM((8 + positions, channels), f32),
            pltpu.VMEM((16, channels), bf16),
            pltpu.VMEM((16, channels), bf16),
            pltpu.VMEM((tokens, width), bf16),
            pltpu.VMEM((tokens, width), f32),
            pltpu.SemaphoreType.DMA((13,)),
            pltpu.SemaphoreType.DMA((2,)),
            pltpu.SemaphoreType.DMA,
            pltpu.SemaphoreType.DMA((CHUNKS,)),
            pltpu.SemaphoreType.DMA,
            pltpu.SemaphoreType.DMA((CHUNKS,)),
            pltpu.SemaphoreType.DMA((2,)),
        ],
        compiler_params=pltpu.CompilerParams(
            collective_id=0, has_side_effects=True, vmem_limit_bytes=62 * 2**20
        ),
        name="layer_step",
    )(
        gate_outer,
        gate_inner,
        conv_input,
        conv_taps,
        mixer_out_weight,
        moe_tokens,
        norm_gain.reshape(1, width),
        expert_ids.T,
        route_weight.T,
        offsets,
        expert_gate.reshape(width, hidden),
        expert_up.reshape(width, hidden),
        expert_down.reshape(hidden, width),
    )


def solution(mesh):
    rows = P(("ep", "tp"), None)
    experts = P(("ep", "tp"), None, None)
    in_specs = (rows, rows, rows, P(), P(), rows, P(), rows, rows, experts, experts, experts)
    return jax.shard_map(
        shards, mesh=mesh, in_specs=in_specs, out_specs=(rows, rows), check_vma=False
    )
```

```python
import functools

import jax
import jax.numpy as jnp
from jax import lax
from jax.experimental import pallas as pl
from jax.experimental.pallas import tpu as pltpu
from jax.sharding import PartitionSpec as P

epsilon = 1e-06
clamp_limit = 7.0
alpha_gate = 1.702
MESH = pl.DeviceIdType.MESH

SIDE = 4
CORES = 2


def peer_order():
    def hops(off):
        return sum(min(v, SIDE - v) for v in off[:3])

    offs = [
        (dz, dy, dx, dk)
        for dz in range(SIDE)
        for dy in range(SIDE)
        for dx in range(SIDE)
        for dk in range(CORES)
    ][1:]
    state = 12345
    keyed = []
    for off in offs:
        state = (state * 1103515245 + 12345) % (1 << 31)
        keyed.append((-hops(off), state >> 8, off))
    return [k[2] for k in sorted(keyed)] + [(0, 0, 0, 0)]


ORDER = peer_order()
PEERS = len(ORDER)
GROUP = 8
CHUNK = 16
CHUNKS = PEERS // CHUNK
ROWS = CHUNK * GROUP


def kernel(
    cap,
    go_hbm,
    gi_hbm,
    ci_hbm,
    taps_hbm,
    wmix_hbm,
    tok_hbm,
    gain_hbm,
    ids_hbm,
    rw_hbm,
    wg_hbm,
    wu_hbm,
    wd_hbm,
    mixed,
    moe,
    go,
    gi,
    ci,
    taps,
    wmix,
    tok,
    gain,
    ids,
    rw,
    wg,
    wu,
    wd,
    send,
    recv,
    ret,
    pick,
    comb,
    prod,
    tails,
    tail,
    halo,
    normed,
    acc,
    lsem,
    dsend,
    drecv,
    rsend,
    rrecv,
    hsem,
):
    ep = lax.axis_index("ep")
    tp = lax.axis_index("tp")
    z = ep // (SIDE * CORES)
    y = (ep // CORES) % SIDE
    k = ep % CORES
    x = tp

    def local(i, src, dst):
        copy = pltpu.make_async_copy(src, dst, lsem.at[i])
        copy.start()
        return copy

    positions = gi.shape[0]
    last = pl.ds(positions - 16, 16)
    small = [
        local(0, tok_hbm, tok),
        local(1, ids_hbm, ids),
        local(2, rw_hbm, rw),
        local(3, gain_hbm, gain),
        local(4, gi_hbm.at[last], tails.at[0]),
        local(13, ci_hbm.at[last], tails.at[1]),
    ]

    zs = [(z + d) % SIDE * (SIDE * CORES) for d in range(SIDE)]
    zn = [(z + SIDE - d) % SIDE * (SIDE * CORES) for d in range(SIDE)]
    ys = [(y + d) % SIDE * CORES for d in range(SIDE)]
    yn = [(y + SIDE - d) % SIDE * CORES for d in range(SIDE)]
    xs = [(x + d) % SIDE for d in range(SIDE)]
    xn = [(x + SIDE - d) % SIDE for d in range(SIDE)]
    ks = [(k + d) % CORES for d in range(CORES)]

    def ahead(i):
        dz, dy, dx, dk = ORDER[i]
        return (zs[dz] + ys[dy] + ks[dk], xs[dx])

    def behind(i):
        dz, dy, dx, dk = ORDER[i]
        return (zn[dz] + yn[dy] + ks[dk], xn[dx])

    barrier = pltpu.get_barrier_semaphore()
    for i in range(PEERS - 1):
        pl.semaphore_signal(barrier, inc=1, device_id=ahead(i), device_id_type=MESH)

    mix_in = [
        local(5, gi_hbm, gi),
        local(6, ci_hbm, ci),
        local(7, go_hbm, go),
        local(8, taps_hbm, taps),
        local(9, wmix_hbm, wmix),
    ]
    experts_in = [
        local(10, wg_hbm, wg),
        local(11, wu_hbm, wu),
        local(12, wd_hbm, wd),
    ]

    for copy in small:
        copy.wait()
    wide = tok[...].astype(jnp.float32)
    mean = jnp.mean(wide * wide, axis=-1, keepdims=True)
    normed[...] = (wide * lax.rsqrt(mean + epsilon) * gain[...]).astype(jnp.bfloat16)

    tail[...] = (tails[0].astype(jnp.float32) * tails[1].astype(jnp.float32)).astype(jnp.bfloat16)
    here = ep * SIDE + tp
    after = (here + 1) % PEERS
    halo_copy = pltpu.make_async_remote_copy(
        tail.at[pl.ds(8, 8)],
        halo.at[pl.ds(8, 8)],
        hsem.at[0],
        hsem.at[1],
        device_id=(after // SIDE, after % SIDE),
        device_id_type=MESH,
    )

    tokens = tok.shape[0]
    sublane = lax.broadcasted_iota(jnp.int32, (GROUP, tokens), 0)
    off = []
    for i in range(0, PEERS, GROUP):
        codes = [dz * 32 + dy * 8 + dk * 4 + dx for dz, dy, dx, dk in ORDER[i : i + GROUP]]
        part = jnp.full((GROUP, tokens), codes[0], jnp.int32)
        for j in range(1, GROUP):
            part = jnp.where(sublane == j, codes[j], part)
        off.append(part)
    off = jnp.concatenate(off, axis=0)
    oz, oy, ok, ox = off // 32, (off // 8) % SIDE, (off // 4) % CORES, off % SIDE
    target = (
        (z + oz) % SIDE * 32 + (y + oy) % SIDE * 8 + (k + ok) % CORES * 4 + (x + ox) % SIDE
    )
    weights = rw[...]
    weights = weights / jnp.sum(weights, axis=0, keepdims=True)
    named = jnp.zeros((PEERS, tokens), jnp.float32)
    named_weight = jnp.zeros((PEERS, tokens), jnp.float32)
    for j in range(ids.shape[0]):
        hit = ids[j : j + 1, :] == target
        named = jnp.where(hit, 1.0, named)
        named_weight = jnp.where(hit, weights[j : j + 1, :], named_weight)
    earlier = (
        lax.broadcasted_iota(jnp.int32, (tokens, tokens), 0)
        < lax.broadcasted_iota(jnp.int32, (tokens, tokens), 1)
    ).astype(jnp.bfloat16)
    rank = jnp.dot(named.astype(jnp.bfloat16), earlier, preferred_element_type=jnp.float32)
    rank = jnp.where(named > 0.5, rank, 99.0)
    place = lax.broadcasted_iota(jnp.int32, (PEERS, GROUP, tokens), 1).astype(jnp.float32)
    chosen = jnp.broadcast_to(rank[:, None, :], (PEERS, GROUP, tokens)) == place
    pick[...] = (
        jnp.where(chosen, 1.0, 0.0).reshape(PEERS * GROUP, tokens).astype(jnp.bfloat16)
    )

    def dispatch(i):
        rows = pl.ds(i * GROUP, cap)
        return pltpu.make_async_remote_copy(
            send.at[rows],
            recv.at[rows],
            dsend,
            drecv.at[i // CHUNK],
            device_id=ahead(i),
            device_id_type=MESH,
        )

    def giveback(i):
        rows = pl.ds(i * GROUP, cap)
        return pltpu.make_async_remote_copy(
            recv.at[rows],
            ret.at[rows],
            rsend,
            rrecv.at[i // CHUNK],
            device_id=behind(i),
            device_id_type=MESH,
        )

    def peers_of(c):
        return range(c * CHUNK, min((c + 1) * CHUNK, PEERS - 1))

    def all_rows(ref, sem, count):
        part = ref.at[pl.ds(0, count * GROUP), pl.ds(0, ref.shape[1] * cap // GROUP)]
        return pltpu.make_async_copy(part, part, sem)

    for c in range(CHUNKS):
        rows = pl.ds(c * ROWS, ROWS)
        send[rows, :] = jnp.dot(
            pick[rows, :], normed[...], preferred_element_type=jnp.float32
        ).astype(jnp.bfloat16)
        if c == 0:
            with jax.named_scope("barrier"):
                pl.semaphore_wait(barrier, PEERS - 1)
            halo_copy.start()
        else:
            for i in peers_of(c - 1):
                dispatch(i).start()
    for i in peers_of(CHUNKS - 1):
        dispatch(i).start()
    own = pl.ds((PEERS - 1) * GROUP, GROUP)
    recv[own, :] = send[own, :]

    reach = taps.shape[0] - 1
    for copy in mix_in[:2]:
        copy.wait()
    block = 128

    @pl.loop(0, positions // block)
    def _(b):
        rows = pl.ds(pl.multiple_of(b * block, block), block)
        prod[pl.ds(pl.multiple_of(8 + b * block, 8), block), :] = (
            (gi[rows, :].astype(jnp.float32) * ci[rows, :].astype(jnp.float32))
            .astype(jnp.bfloat16)
            .astype(jnp.float32)
        )

    for c in range(CHUNKS):
        group = rank[c * CHUNK : (c + 1) * CHUNK]
        group_weight = named_weight[c * CHUNK : (c + 1) * CHUNK]
        shape = (CHUNK, GROUP, tokens)
        share = jnp.where(
            jnp.broadcast_to(group[:, None, :], shape) == place[:CHUNK],
            jnp.broadcast_to(group_weight[:, None, :], shape),
            0.0,
        ).reshape(ROWS, tokens)
        comb[c] = share.T.astype(jnp.bfloat16)

    for copy in mix_in[2:]:
        copy.wait()
    with jax.named_scope('halo_wait'):
        halo_copy.wait()
    prod[0:8, :] = jnp.where(here == 0, 0.0, halo[8:16, :].astype(jnp.float32))

    @pl.loop(0, positions // block)
    def _(b):
        rows = pl.ds(pl.multiple_of(b * block, block), block)
        window = prod[pl.ds(pl.multiple_of(b * block, 8), block + 8), :]
        convolved = jnp.zeros((block, window.shape[1]), jnp.float32)
        for j in range(reach + 1):
            start = 8 - reach + j
            convolved = convolved + taps[j : j + 1, :] * window[start : start + block]
        gated = (go[rows, :].astype(jnp.float32) * convolved).astype(jnp.bfloat16)
        mixed[rows, :] = jnp.dot(
            gated, wmix[...], preferred_element_type=jnp.float32
        ).astype(jnp.bfloat16)

    with jax.named_scope('expw_wait'):
        for copy in experts_in:
            copy.wait()

    @pl.loop(0, CHUNKS)
    def _(c):
        for n in range(CHUNKS):

            @pl.when(c == n)
            def _():
                with jax.named_scope('dwait'):
                    all_rows(recv, drecv.at[n], len(peers_of(n))).wait()

        rows = pl.ds(pl.multiple_of(c * ROWS, ROWS), ROWS)
        block_rows = recv[rows, :]
        hidden = []
        width = 256
        for n in range(0, wg.shape[1], width):
            gate_pre = jnp.dot(
                block_rows, wg[:, n : n + width], preferred_element_type=jnp.float32
            )
            up_pre = jnp.dot(
                block_rows, wu[:, n : n + width], preferred_element_type=jnp.float32
            )
            gate_pre = jnp.minimum(gate_pre, clamp_limit)
            up_pre = jnp.clip(up_pre, -clamp_limit, clamp_limit)
            hidden.append(
                ((up_pre + 1.0) * (gate_pre * jax.nn.sigmoid(alpha_gate * gate_pre))).astype(
                    jnp.bfloat16
                )
            )
        hidden = jnp.concatenate(hidden, axis=1)
        for n in range(0, wd.shape[1], width):
            recv[rows, n : n + width] = jnp.dot(
                hidden, wd[:, n : n + width], preferred_element_type=jnp.float32
            ).astype(jnp.bfloat16)
        for n in range(CHUNKS):

            @pl.when(c == n)
            def _():
                for i in peers_of(n):
                    giveback(i).start()

    ret[own, :] = recv[own, :]

    acc[...] = jnp.zeros_like(acc)
    used = lax.broadcasted_iota(jnp.int32, (ROWS, ret.shape[1]), 0) % GROUP < cap

    @pl.loop(0, CHUNKS)
    def _(c):
        for n in range(CHUNKS):

            @pl.when(c == n)
            def _():
                with jax.named_scope('rwait'):
                    all_rows(ret, rrecv.at[n], len(peers_of(n))).wait()

        rows = pl.ds(pl.multiple_of(c * ROWS, ROWS), ROWS)
        back = jnp.where(used, ret[rows, :].astype(jnp.float32), 0.0).astype(jnp.bfloat16)
        acc[...] += jnp.dot(comb[c], back, preferred_element_type=jnp.float32)

    moe[...] = acc[...].astype(jnp.bfloat16)
    with jax.named_scope('endwait'):
        all_rows(send, dsend, PEERS - 1).wait()
        all_rows(recv, rsend, PEERS - 1).wait()


def shards(
    gate_outer,
    gate_inner,
    conv_input,
    conv_taps,
    mixer_out_weight,
    moe_tokens,
    norm_gain,
    expert_ids,
    route_weight,
    expert_gate,
    expert_up,
    expert_down,
):
    positions, channels = gate_inner.shape
    tokens, width = moe_tokens.shape
    hidden = expert_gate.shape[2]
    choices = expert_ids.shape[1]
    cap = 3 * tokens * choices // (2 * PEERS)
    bf16, f32 = jnp.bfloat16, jnp.float32
    anywhere = pl.BlockSpec(memory_space=pl.ANY)
    slots = (PEERS * GROUP, width)
    return pl.pallas_call(
        functools.partial(kernel, cap),
        out_shape=(
            pltpu.VMEM((positions, width), bf16),
            pltpu.VMEM((tokens, width), bf16),
        ),
        in_specs=[anywhere] * 12,
        out_specs=(pl.BlockSpec(memory_space=pltpu.VMEM), pl.BlockSpec(memory_space=pltpu.VMEM)),
        scratch_shapes=[
            pltpu.VMEM((positions, channels), bf16),
            pltpu.VMEM((positions, channels), bf16),
            pltpu.VMEM((positions, channels), bf16),
            pltpu.VMEM(conv_taps.shape, f32),
            pltpu.VMEM((channels, width), bf16),
            pltpu.VMEM((tokens, width), bf16),
            pltpu.VMEM((1, width), f32),
            pltpu.VMEM((choices, tokens), jnp.int32),
            pltpu.VMEM((choices, tokens), f32),
            pltpu.VMEM((width, hidden), bf16),
            pltpu.VMEM((width, hidden), bf16),
            pltpu.VMEM((hidden, width), bf16),
            pltpu.VMEM(slots, bf16),
            pltpu.VMEM(slots, bf16),
            pltpu.VMEM(slots, bf16),
            pltpu.VMEM((PEERS * GROUP, tokens), bf16),
            pltpu.VMEM((CHUNKS, tokens, ROWS), bf16),
            pltpu.VMEM((8 + positions, channels), f32),
            pltpu.VMEM((2, 16, channels), bf16),
            pltpu.VMEM((16, channels), bf16),
            pltpu.VMEM((16, channels), bf16),
            pltpu.VMEM((tokens, width), bf16),
            pltpu.VMEM((tokens, width), f32),
            pltpu.SemaphoreType.DMA((14,)),
            pltpu.SemaphoreType.DMA,
            pltpu.SemaphoreType.DMA((CHUNKS,)),
            pltpu.SemaphoreType.DMA,
            pltpu.SemaphoreType.DMA((CHUNKS,)),
            pltpu.SemaphoreType.DMA((2,)),
        ],
        compiler_params=pltpu.CompilerParams(
            collective_id=0, has_side_effects=True, vmem_limit_bytes=56 * 2**20
        ),
        name="layer_step",
    )(
        gate_outer,
        gate_inner,
        conv_input,
        conv_taps,
        mixer_out_weight,
        moe_tokens,
        norm_gain.reshape(1, width),
        expert_ids.T,
        route_weight.T,
        expert_gate.reshape(width, hidden),
        expert_up.reshape(width, hidden),
        expert_down.reshape(hidden, width),
    )


def solution(mesh):
    rows = P(("ep", "tp"), None)
    experts = P(("ep", "tp"), None, None)
    in_specs = (rows, rows, rows, P(), P(), rows, P(), rows, rows, experts, experts, experts)
    return jax.shard_map(
        shards, mesh=mesh, in_specs=in_specs, out_specs=(rows, rows), check_vma=False
    )
```

```python
import functools

import jax
import jax.numpy as jnp
from jax import lax
from jax.experimental import pallas as pl
from jax.experimental.pallas import tpu as pltpu
from jax.sharding import PartitionSpec as P

epsilon = 1e-06
clamp_limit = 7.0
alpha_gate = 1.702
MESH = pl.DeviceIdType.MESH

SIDE = 4
CORES = 2
AXES = 3


def hops(off):
    return sum(min(v, SIDE - v) for v in off[:AXES])


def shuffled(offs, rank_of):
    state = 12345
    keyed = []
    for off in offs:
        state = (state * 1103515245 + 12345) % (1 << 31)
        keyed.append((rank_of(off), state >> 8, off))
    return [k[2] for k in sorted(keyed)]


EVERY = [
    (dz, dy, dx, dk)
    for dz in range(SIDE)
    for dy in range(SIDE)
    for dx in range(SIDE)
    for dk in range(CORES)
]
SELF = (0, 0, 0, 0)
ORDER = shuffled(EVERY[1:], lambda off: 2 in off[:AXES]) + [SELF]
PEERS = len(ORDER)
SLOT = {off: i for i, off in enumerate(ORDER)}
FAR = shuffled(EVERY[1:], lambda off: -hops(off))
PLANE = [shuffled([o for o in EVERY[1:] if o[a] == 0], lambda off: -hops(off)) + [SELF] for a in range(AXES)]
GROUP = 8
CHUNK = 16
CHUNKS = PEERS // CHUNK
ROWS = CHUNK * GROUP
LINE = PEERS // SIDE


def kernel(
    cap,
    go_hbm,
    gi_hbm,
    ci_hbm,
    taps_hbm,
    wmix_hbm,
    tok_hbm,
    gain_hbm,
    ids_hbm,
    rw_hbm,
    wg_hbm,
    wu_hbm,
    wd_hbm,
    mixed,
    moe,
    go,
    gi,
    ci,
    taps,
    wmix,
    tok,
    gain,
    ids,
    rw,
    wg,
    wu,
    wd,
    send,
    recv,
    ret,
    gath,
    idsg,
    comb,
    prod,
    tails,
    tail,
    halo,
    normed,
    acc,
    lsem,
    gsend,
    grecv,
    isend,
    irecv,
    dsend,
    drecv,
    rsend,
    rrecv,
    hsem,
):
    ep = lax.axis_index("ep")
    tp = lax.axis_index("tp")
    z = ep // (SIDE * CORES)
    y = (ep // CORES) % SIDE
    k = ep % CORES
    x = tp

    def local(i, src, dst):
        copy = pltpu.make_async_copy(src, dst, lsem.at[i])
        copy.start()
        return copy

    positions = gi.shape[0]
    last = pl.ds(positions - 16, 16)
    small = [
        local(0, tok_hbm, tok),
        local(1, ids_hbm, ids),
        local(2, rw_hbm, rw),
        local(3, gain_hbm, gain),
        local(4, gi_hbm.at[last], tails.at[0]),
        local(13, ci_hbm.at[last], tails.at[1]),
    ]

    zs = [(z + d) % SIDE * (SIDE * CORES) for d in range(SIDE)]
    zn = [(z + SIDE - d) % SIDE * (SIDE * CORES) for d in range(SIDE)]
    ys = [(y + d) % SIDE * CORES for d in range(SIDE)]
    yn = [(y + SIDE - d) % SIDE * CORES for d in range(SIDE)]
    xs = [(x + d) % SIDE for d in range(SIDE)]
    xn = [(x + SIDE - d) % SIDE for d in range(SIDE)]
    ks = [(k + d) % CORES for d in range(CORES)]

    def ahead(off):
        dz, dy, dx, dk = off
        return (zs[dz] + ys[dy] + ks[dk], xs[dx])

    def behind(i):
        dz, dy, dx, dk = ORDER[i]
        return (zn[dz] + yn[dy] + ks[dk], xn[dx])

    barrier = pltpu.get_barrier_semaphore()
    for off in FAR:
        pl.semaphore_signal(barrier, inc=1, device_id=ahead(off), device_id_type=MESH)

    mix_in = [
        local(5, gi_hbm, gi),
        local(6, ci_hbm, ci),
        local(7, go_hbm, go),
        local(8, taps_hbm, taps),
        local(9, wmix_hbm, wmix),
    ]
    experts_in = [
        local(10, wg_hbm, wg),
        local(11, wu_hbm, wu),
        local(12, wd_hbm, wd),
    ]

    for copy in small:
        copy.wait()
    wide = tok[...].astype(jnp.float32)
    mean = jnp.mean(wide * wide, axis=-1, keepdims=True)
    normed[...] = (wide * lax.rsqrt(mean + epsilon) * gain[...]).astype(jnp.bfloat16)

    tail[...] = (tails[0].astype(jnp.float32) * tails[1].astype(jnp.float32)).astype(jnp.bfloat16)
    here = ep * SIDE + tp
    after = (here + 1) % PEERS
    halo_copy = pltpu.make_async_remote_copy(
        tail.at[pl.ds(8, 8)],
        halo.at[pl.ds(8, 8)],
        hsem.at[0],
        hsem.at[1],
        device_id=(after // SIDE, after % SIDE),
        device_id_type=MESH,
    )

    tokens = tok.shape[0]
    width = tok.shape[1]
    sublane = lax.broadcasted_iota(jnp.int32, (GROUP, tokens), 0)
    earlier = (
        lax.broadcasted_iota(jnp.int32, (tokens, tokens), 0)
        < lax.broadcasted_iota(jnp.int32, (tokens, tokens), 1)
    ).astype(jnp.bfloat16)
    place = lax.broadcasted_iota(jnp.int32, (CHUNK, GROUP, tokens), 1).astype(jnp.float32)

    def experts_at(offs):
        parts = []
        for i in range(0, len(offs), GROUP):
            codes = [dz * 32 + dy * 8 + dk * 4 + dx for dz, dy, dx, dk in offs[i : i + GROUP]]
            part = jnp.full((GROUP, tokens), codes[0], jnp.int32)
            for j in range(1, GROUP):
                part = jnp.where(sublane == j, codes[j], part)
            parts.append(part)
        off = jnp.concatenate(parts, axis=0)
        oz, oy, ok, ox = off // 32, (off // 8) % SIDE, (off // 4) % CORES, off % SIDE
        return (z + oz) % SIDE * 32 + (y + oy) % SIDE * 8 + (k + ok) % CORES * 4 + (x + ox) % SIDE

    def ranks(named):
        rank = jnp.dot(named.astype(jnp.bfloat16), earlier, preferred_element_type=jnp.float32)
        return jnp.where(named > 0.5, rank, 99.0)

    def named_by(listing, target):
        named = jnp.zeros(target.shape, jnp.float32)
        for j in range(ids.shape[0]):
            named = jnp.where(listing[j : j + 1, :] == target, 1.0, named)
        return named

    lanes = width // 128
    cuts = [lanes // AXES * p * 128 for p in range(AXES)] + [width]

    def columns(p):
        return pl.ds(cuts[p], cuts[p + 1] - cuts[p])

    def along(p, d):
        return tuple(d if a == p else 0 for a in range(AXES)) + (0,)

    def line(p, d):
        return pltpu.make_async_remote_copy(
            normed.at[:, columns(p)],
            gath.at[d - 1, :, columns(p)],
            gsend,
            grecv.at[p * 4 + d - 1],
            device_id=ahead(along(p, d)),
            device_id_type=MESH,
        )

    def relay(p, d):
        rows = pl.ds(0 if d == 1 else tokens // 2, tokens // 2)
        return pltpu.make_async_remote_copy(
            gath.at[d - 1, rows, columns(p)],
            gath.at[1, rows, columns(p)],
            gsend,
            grecv.at[p * 4 + (1 if d == 1 else 3)],
            device_id=ahead(along(p, d)),
            device_id_type=MESH,
        )

    def listing(p, d):
        n = p * (SIDE - 1) + d - 1
        return pltpu.make_async_remote_copy(
            ids,
            idsg.at[n],
            isend.at[n],
            irecv.at[n],
            device_id=ahead(along(p, d)),
            device_id_type=MESH,
        )

    def dispatch(p, d, i):
        off = PLANE[p][i]
        slot = SLOT[tuple(d if a == p else off[a] for a in range(AXES)) + off[AXES:]]
        source = send.at[pl.ds((d * LINE + i) * GROUP, cap), columns(p)]
        target = recv.at[pl.ds(slot * GROUP, cap), columns(p)]
        if off == SELF:
            return pltpu.make_async_copy(source, target, drecv.at[slot // CHUNK])
        return pltpu.make_async_remote_copy(
            source,
            target,
            dsend,
            drecv.at[slot // CHUNK],
            device_id=ahead(off),
            device_id_type=MESH,
        )

    def giveback(i):
        rows = pl.ds(i * GROUP, cap)
        return pltpu.make_async_remote_copy(
            recv.at[rows],
            ret.at[rows],
            rsend,
            rrecv.at[i // CHUNK],
            device_id=behind(i),
            device_id_type=MESH,
        )

    def peers_of(c):
        return range(c * CHUNK, min((c + 1) * CHUNK, PEERS - 1))

    def all_rows(ref, sem, count):
        part = ref.at[pl.ds(0, count * GROUP), pl.ds(0, ref.shape[1] * cap // GROUP)]
        return pltpu.make_async_copy(part, part, sem)

    targets = [experts_at(PLANE[p]) for p in range(AXES)]
    with jax.named_scope("barrier"):
        pl.semaphore_wait(barrier, PEERS - 1)
    halo_copy.start()
    near = (1, SIDE - 1)
    listings = [listing(p, d) for d in range(1, SIDE) for p in range(AXES)]
    for copy in listings:
        copy.start()
    for d in near:
        for p in range(AXES):
            line(p, d).start()

    waiting = []

    def pick_rows(p, d):
        if d == 0:
            listed, rows_of = ids[...], normed[:, cuts[p] : cuts[p + 1]]
        else:
            listed = idsg[p * (SIDE - 1) + d - 1]
            rows_of = gath[d - 1, :, cuts[p] : cuts[p + 1]]
        rank = ranks(named_by(listed, targets[p]))
        for h in range(0, LINE, CHUNK):
            group = jnp.broadcast_to(rank[h : h + CHUNK][:, None, :], place.shape)
            pick = jnp.where(group == place, 1.0, 0.0).reshape(ROWS, tokens).astype(jnp.bfloat16)
            send[pl.ds((d * LINE + h) * GROUP, ROWS), cuts[p] : cuts[p + 1]] = jnp.dot(
                pick, rows_of, preferred_element_type=jnp.float32
            ).astype(jnp.bfloat16)
            for copy in waiting:
                copy.start()
            waiting[:] = [dispatch(p, d, i) for i in range(h, h + CHUNK)]

    for p in range(AXES):
        pick_rows(p, 0)
    with jax.named_scope("listwait"):
        for copy in listings:
            copy.wait()
    for d in near:
        for p in range(AXES):
            with jax.named_scope("linewait"):
                line(p, d).wait_recv()
            relay(p, d).start()
    for d in near:
        for p in range(AXES):
            pick_rows(p, d)
    for copy in waiting:
        copy.start()
    waiting.clear()
    reach = taps.shape[0] - 1
    for copy in mix_in[:2]:
        copy.wait()
    block = 128

    @pl.loop(0, positions // block)
    def _(b):
        rows = pl.ds(pl.multiple_of(b * block, block), block)
        prod[pl.ds(pl.multiple_of(8 + b * block, 8), block), :] = (
            (gi[rows, :].astype(jnp.float32) * ci[rows, :].astype(jnp.float32))
            .astype(jnp.bfloat16)
            .astype(jnp.float32)
        )

    for copy in mix_in[2:]:
        copy.wait()
    with jax.named_scope('halo_wait'):
        halo_copy.wait()
    prod[0:8, :] = jnp.where(here == 0, 0.0, halo[8:16, :].astype(jnp.float32))

    @pl.loop(0, positions // block)
    def _(b):
        rows = pl.ds(pl.multiple_of(b * block, block), block)
        window = prod[pl.ds(pl.multiple_of(b * block, 8), block + 8), :]
        convolved = jnp.zeros((block, window.shape[1]), jnp.float32)
        for j in range(reach + 1):
            start = 8 - reach + j
            convolved = convolved + taps[j : j + 1, :] * window[start : start + block]
        gated = (go[rows, :].astype(jnp.float32) * convolved).astype(jnp.bfloat16)
        mixed[rows, :] = jnp.dot(
            gated, wmix[...], preferred_element_type=jnp.float32
        ).astype(jnp.bfloat16)

    for p in range(AXES):
        with jax.named_scope("relaywait"):
            for d in near:
                relay(p, d).wait_recv()
        pick_rows(p, 2)
    for copy in waiting:
        copy.start()

    with jax.named_scope('expw_wait'):
        for copy in experts_in:
            copy.wait()

    @pl.loop(0, CHUNKS)
    def _(c):
        for n in range(CHUNKS):

            @pl.when(c == n)
            def _():
                with jax.named_scope('dwait'):
                    all_rows(recv, drecv.at[n], CHUNK).wait()

        rows = pl.ds(pl.multiple_of(c * ROWS, ROWS), ROWS)
        block_rows = recv[rows, :]
        hidden = []
        width = 256
        for n in range(0, wg.shape[1], width):
            gate_pre = jnp.dot(
                block_rows, wg[:, n : n + width], preferred_element_type=jnp.float32
            )
            up_pre = jnp.dot(
                block_rows, wu[:, n : n + width], preferred_element_type=jnp.float32
            )
            gate_pre = jnp.minimum(gate_pre, clamp_limit)
            up_pre = jnp.clip(up_pre, -clamp_limit, clamp_limit)
            hidden.append(
                ((up_pre + 1.0) * (gate_pre * jax.nn.sigmoid(alpha_gate * gate_pre))).astype(
                    jnp.bfloat16
                )
            )
        hidden = jnp.concatenate(hidden, axis=1)
        for n in range(0, wd.shape[1], width):
            recv[rows, n : n + width] = jnp.dot(
                hidden, wd[:, n : n + width], preferred_element_type=jnp.float32
            ).astype(jnp.bfloat16)
        for n in range(CHUNKS):

            @pl.when(c == n)
            def _():
                for i in peers_of(n):
                    giveback(i).start()

    own = pl.ds((PEERS - 1) * GROUP, GROUP)
    ret[own, :] = recv[own, :]

    weights = rw[...]
    weights = weights / jnp.sum(weights, axis=0, keepdims=True)
    target = experts_at(ORDER)
    rank = ranks(named_by(ids[...], target))
    named_weight = jnp.zeros(target.shape, jnp.float32)
    for j in range(ids.shape[0]):
        named_weight = jnp.where(ids[j : j + 1, :] == target, weights[j : j + 1, :], named_weight)

    for c in range(CHUNKS):
        group = rank[c * CHUNK : (c + 1) * CHUNK]
        group_weight = named_weight[c * CHUNK : (c + 1) * CHUNK]
        shape = (CHUNK, GROUP, tokens)
        share = jnp.where(
            jnp.broadcast_to(group[:, None, :], shape) == place,
            jnp.broadcast_to(group_weight[:, None, :], shape),
            0.0,
        ).reshape(ROWS, tokens)
        comb[c] = share.T.astype(jnp.bfloat16)


    acc[...] = jnp.zeros_like(acc)
    used = lax.broadcasted_iota(jnp.int32, (ROWS, ret.shape[1]), 0) % GROUP < cap

    @pl.loop(0, CHUNKS)
    def _(c):
        for n in range(CHUNKS):

            @pl.when(c == n)
            def _():
                with jax.named_scope('rwait'):
                    all_rows(ret, rrecv.at[n], len(peers_of(n))).wait()

        rows = pl.ds(pl.multiple_of(c * ROWS, ROWS), ROWS)
        back = jnp.where(used, ret[rows, :].astype(jnp.float32), 0.0).astype(jnp.bfloat16)
        acc[...] += jnp.dot(comb[c], back, preferred_element_type=jnp.float32)

    moe[...] = acc[...].astype(jnp.bfloat16)
    with jax.named_scope('endwait'):
        all_rows(send, dsend, SIDE * (LINE - 1)).wait()
        pltpu.make_async_copy(gath, gath, gsend).wait()
        all_rows(recv, rsend, PEERS - 1).wait()


def shards(
    gate_outer,
    gate_inner,
    conv_input,
    conv_taps,
    mixer_out_weight,
    moe_tokens,
    norm_gain,
    expert_ids,
    route_weight,
    expert_gate,
    expert_up,
    expert_down,
):
    positions, channels = gate_inner.shape
    tokens, width = moe_tokens.shape
    hidden = expert_gate.shape[2]
    choices = expert_ids.shape[1]
    cap = 3 * tokens * choices // (2 * PEERS)
    bf16, f32 = jnp.bfloat16, jnp.float32
    anywhere = pl.BlockSpec(memory_space=pl.ANY)
    slots = (PEERS * GROUP, width)
    return pl.pallas_call(
        functools.partial(kernel, cap),
        out_shape=(
            pltpu.VMEM((positions, width), bf16),
            pltpu.VMEM((tokens, width), bf16),
        ),
        in_specs=[anywhere] * 12,
        out_specs=(pl.BlockSpec(memory_space=pltpu.VMEM), pl.BlockSpec(memory_space=pltpu.VMEM)),
        scratch_shapes=[
            pltpu.VMEM((positions, channels), bf16),
            pltpu.VMEM((positions, channels), bf16),
            pltpu.VMEM((positions, channels), bf16),
            pltpu.VMEM(conv_taps.shape, f32),
            pltpu.VMEM((channels, width), bf16),
            pltpu.VMEM((tokens, width), bf16),
            pltpu.VMEM((1, width), f32),
            pltpu.VMEM((choices, tokens), jnp.int32),
            pltpu.VMEM((choices, tokens), f32),
            pltpu.VMEM((width, hidden), bf16),
            pltpu.VMEM((width, hidden), bf16),
            pltpu.VMEM((hidden, width), bf16),
            pltpu.VMEM(slots, bf16),
            pltpu.VMEM(slots, bf16),
            pltpu.VMEM(slots, bf16),
            pltpu.VMEM((SIDE - 1, tokens, width), bf16),
            pltpu.VMEM((AXES * (SIDE - 1), choices, tokens), jnp.int32),
            pltpu.VMEM((CHUNKS, tokens, ROWS), bf16),
            pltpu.VMEM((8 + positions, channels), f32),
            pltpu.VMEM((2, 16, channels), bf16),
            pltpu.VMEM((16, channels), bf16),
            pltpu.VMEM((16, channels), bf16),
            pltpu.VMEM((tokens, width), bf16),
            pltpu.VMEM((tokens, width), f32),
            pltpu.SemaphoreType.DMA((14,)),
            pltpu.SemaphoreType.DMA,
            pltpu.SemaphoreType.DMA((4 * AXES,)),
            pltpu.SemaphoreType.DMA((AXES * (SIDE - 1),)),
            pltpu.SemaphoreType.DMA((AXES * (SIDE - 1),)),
            pltpu.SemaphoreType.DMA,
            pltpu.SemaphoreType.DMA((CHUNKS,)),
            pltpu.SemaphoreType.DMA,
            pltpu.SemaphoreType.DMA((CHUNKS,)),
            pltpu.SemaphoreType.DMA((2,)),
        ],
        compiler_params=pltpu.CompilerParams(
            collective_id=0, has_side_effects=True, vmem_limit_bytes=56 * 2**20
        ),
        name="layer_step",
    )(
        gate_outer,
        gate_inner,
        conv_input,
        conv_taps,
        mixer_out_weight,
        moe_tokens,
        norm_gain.reshape(1, width),
        expert_ids.T,
        route_weight.T,
        expert_gate.reshape(width, hidden),
        expert_up.reshape(width, hidden),
        expert_down.reshape(hidden, width),
    )


def solution(mesh):
    rows = P(("ep", "tp"), None)
    experts = P(("ep", "tp"), None, None)
    in_specs = (rows, rows, rows, P(), P(), rows, P(), rows, rows, experts, experts, experts)
    return jax.shard_map(
        shards, mesh=mesh, in_specs=in_specs, out_specs=(rows, rows), check_vma=False
    )
```

```python
import functools

import jax
import jax.numpy as jnp
from jax import lax
from jax.experimental import pallas as pl
from jax.experimental.pallas import tpu as pltpu
from jax.sharding import PartitionSpec as P

epsilon = 1e-06
clamp_limit = 7.0
alpha_gate = 1.702
MESH = pl.DeviceIdType.MESH

SIDE = 4
CORES = 2
AXES = 3


def hops(off):
    return sum(min(v, SIDE - v) for v in off[:AXES])


def shuffled(offs, rank_of):
    state = 12345
    keyed = []
    for off in offs:
        state = (state * 1103515245 + 12345) % (1 << 31)
        keyed.append((rank_of(off), state >> 8, off))
    return [k[2] for k in sorted(keyed)]


EVERY = [
    (dz, dy, dx, dk)
    for dz in range(SIDE)
    for dy in range(SIDE)
    for dx in range(SIDE)
    for dk in range(CORES)
]
SELF = (0, 0, 0, 0)
BLOCKS = (2, 1, 3)
ORDER = shuffled(EVERY, lambda off: (off == SELF, 2 in off[:AXES]))
PEERS = len(ORDER)
SLOT = {off: i for i, off in enumerate(ORDER)}
FAR = shuffled(EVERY[1:], lambda off: -hops(off))
PLANE = [shuffled([o for o in EVERY[1:] if o[a] == 0], lambda off: -hops(off)) + [SELF] for a in range(AXES)]
GROUP = 8
CHUNK = 16
TILE = 16
TILES = PEERS // TILE
ROWS = CHUNK * GROUP
LINE = PEERS // SIDE


def kernel(
    cap,
    go_hbm,
    gi_hbm,
    ci_hbm,
    taps_hbm,
    wmix_hbm,
    tok_hbm,
    gain_hbm,
    ids_hbm,
    rw_hbm,
    wg_hbm,
    wu_hbm,
    wd_hbm,
    mixed,
    moe,
    go,
    gi,
    ci,
    taps,
    wmix,
    tok,
    gain,
    ids,
    rw,
    wg,
    wu,
    wd,
    send,
    recv,
    ret,
    gath,
    facts,
    factg,
    ranked,
    shared,
    part,
    back,
    comb,
    prod,
    tails,
    tail,
    halo,
    normed,
    acc,
    lsem,
    gsend,
    grecv,
    isend,
    irecv,
    dsend,
    drecv,
    rsend,
    rrecv,
    bsend,
    brecv,
    hsem,
):
    ep = lax.axis_index("ep")
    tp = lax.axis_index("tp")
    z = ep // (SIDE * CORES)
    y = (ep // CORES) % SIDE
    k = ep % CORES
    x = tp

    def local(i, src, dst):
        copy = pltpu.make_async_copy(src, dst, lsem.at[i])
        copy.start()
        return copy

    positions = gi.shape[0]
    last = pl.ds(positions - 16, 16)
    small = [
        local(0, tok_hbm, tok),
        local(1, ids_hbm, ids),
        local(2, rw_hbm, rw),
        local(3, gain_hbm, gain),
        local(4, gi_hbm.at[last], tails.at[0]),
        local(13, ci_hbm.at[last], tails.at[1]),
    ]

    zs = [(z + d) % SIDE * (SIDE * CORES) for d in range(SIDE)]
    zn = [(z + SIDE - d) % SIDE * (SIDE * CORES) for d in range(SIDE)]
    ys = [(y + d) % SIDE * CORES for d in range(SIDE)]
    yn = [(y + SIDE - d) % SIDE * CORES for d in range(SIDE)]
    xs = [(x + d) % SIDE for d in range(SIDE)]
    xn = [(x + SIDE - d) % SIDE for d in range(SIDE)]
    ks = [(k + d) % CORES for d in range(CORES)]

    def ahead(off):
        dz, dy, dx, dk = off
        return (zs[dz] + ys[dy] + ks[dk], xs[dx])

    def behind(off):
        dz, dy, dx, dk = off
        return (zn[dz] + yn[dy] + ks[dk], xn[dx])

    barrier = pltpu.get_barrier_semaphore()
    for off in FAR:
        pl.semaphore_signal(barrier, inc=1, device_id=ahead(off), device_id_type=MESH)

    mix_in = [
        local(5, gi_hbm, gi),
        local(6, ci_hbm, ci),
        local(7, go_hbm, go),
        local(8, taps_hbm, taps),
        local(9, wmix_hbm, wmix),
    ]
    experts_in = [
        local(10, wg_hbm, wg),
        local(11, wu_hbm, wu),
        local(12, wd_hbm, wd),
    ]

    for copy in small:
        copy.wait()
    wide = tok[...].astype(jnp.float32)
    mean = jnp.mean(wide * wide, axis=-1, keepdims=True)
    normed[...] = (wide * lax.rsqrt(mean + epsilon) * gain[...]).astype(jnp.bfloat16)

    tail[...] = (tails[0].astype(jnp.float32) * tails[1].astype(jnp.float32)).astype(jnp.bfloat16)
    here = ep * SIDE + tp
    after = (here + 1) % PEERS
    halo_copy = pltpu.make_async_remote_copy(
        tail.at[pl.ds(8, 8)],
        halo.at[pl.ds(8, 8)],
        hsem.at[0],
        hsem.at[1],
        device_id=(after // SIDE, after % SIDE),
        device_id_type=MESH,
    )

    tokens = tok.shape[0]
    width = tok.shape[1]
    sublane = lax.broadcasted_iota(jnp.int32, (GROUP, tokens), 0)
    earlier = (
        lax.broadcasted_iota(jnp.int32, (tokens, tokens), 0)
        < lax.broadcasted_iota(jnp.int32, (tokens, tokens), 1)
    ).astype(jnp.bfloat16)
    place = lax.broadcasted_iota(jnp.int32, (CHUNK, GROUP, tokens), 1).astype(jnp.float32)

    def experts_at(offs):
        parts = []
        for i in range(0, len(offs), GROUP):
            codes = [dz * 32 + dy * 8 + dk * 4 + dx for dz, dy, dx, dk in offs[i : i + GROUP]]
            part = jnp.full((GROUP, tokens), codes[0], jnp.int32)
            for j in range(1, GROUP):
                part = jnp.where(sublane == j, codes[j], part)
            parts.append(part)
        off = jnp.concatenate(parts, axis=0)
        oz, oy, ok, ox = off // 32, (off // 8) % SIDE, (off // 4) % CORES, off % SIDE
        return (z + oz) % SIDE * 32 + (y + oy) % SIDE * 8 + (k + ok) % CORES * 4 + (x + ox) % SIDE

    def ranks(named):
        rank = jnp.dot(named.astype(jnp.bfloat16), earlier, preferred_element_type=jnp.float32)
        return jnp.where(named > 0.5, rank, 99.0)

    lanes = width // 128
    cuts = [lanes // AXES * p * 128 for p in range(AXES)] + [width]

    def columns(p):
        return pl.ds(cuts[p], cuts[p + 1] - cuts[p])

    def along(p, d):
        return tuple(d if a == p else 0 for a in range(AXES)) + (0,)

    def line(p, d):
        return pltpu.make_async_remote_copy(
            normed.at[:, columns(p)],
            gath.at[d - 1, :, columns(p)],
            gsend,
            grecv.at[p * 4 + d - 1],
            device_id=ahead(along(p, d)),
            device_id_type=MESH,
        )

    def relay(p, d):
        rows = pl.ds(0 if d == 1 else tokens // 2, tokens // 2)
        return pltpu.make_async_remote_copy(
            gath.at[d - 1, rows, columns(p)],
            gath.at[1, rows, columns(p)],
            gsend,
            grecv.at[p * 4 + (1 if d == 1 else 3)],
            device_id=ahead(along(p, d)),
            device_id_type=MESH,
        )

    def listing(p, d):
        n = p * (SIDE - 1) + d - 1
        return pltpu.make_async_remote_copy(
            facts,
            factg.at[n],
            isend.at[n],
            irecv.at[n],
            device_id=ahead(along(p, d)),
            device_id_type=MESH,
        )

    def dispatch(p, d, i):
        off = PLANE[p][i]
        slot = SLOT[tuple(d if a == p else off[a] for a in range(AXES)) + off[AXES:]]
        source = send.at[pl.ds((d * LINE + i) * GROUP, cap), columns(p)]
        target = recv.at[pl.ds(slot * GROUP, cap), columns(p)]
        if off == SELF:
            return pltpu.make_async_copy(source, target, drecv.at[slot // TILE])
        return pltpu.make_async_remote_copy(
            source,
            target,
            dsend,
            drecv.at[slot // TILE],
            device_id=ahead(off),
            device_id_type=MESH,
        )

    def giveback(p, slot):
        off = ORDER[slot]
        d = off[p]
        flat = tuple(0 if a == p else off[a] for a in range(AXES)) + off[AXES:]
        group = d * LINE + PLANE[p].index(flat)
        source = recv.at[pl.ds(slot * GROUP, cap), columns(p)]
        target = ret.at[pl.ds(group * GROUP, cap), columns(p)]
        if flat == SELF:
            return pltpu.make_async_copy(source, target, rrecv.at[p * SIDE + d])
        return pltpu.make_async_remote_copy(
            source,
            target,
            rsend,
            rrecv.at[p * SIDE + d],
            device_id=behind(flat),
            device_id_type=MESH,
        )

    def partial(p, d):
        return pltpu.make_async_remote_copy(
            part.at[d - 1, :, columns(p)],
            back.at[d - 1, :, columns(p)],
            bsend,
            brecv.at[p * (SIDE - 1) + d - 1],
            device_id=behind(along(p, d)),
            device_id_type=MESH,
        )

    def all_rows(ref, sem, count):
        part = ref.at[pl.ds(0, count * GROUP), pl.ds(0, ref.shape[1] * cap // GROUP)]
        return pltpu.make_async_copy(part, part, sem)

    choices = ids.shape[0]
    weights = rw[...]
    facts[0:choices, :] = ids[...].astype(jnp.float32)
    facts[choices:, :] = weights / jnp.sum(weights, axis=0, keepdims=True)
    targets = [experts_at(PLANE[p]).astype(jnp.float32) for p in range(AXES)]
    with jax.named_scope("barrier"):
        pl.semaphore_wait(barrier, PEERS - 1)
    halo_copy.start()
    near = (1, SIDE - 1)
    listings = [listing(p, d) for d in range(1, SIDE) for p in range(AXES)]
    for copy in listings:
        copy.start()
    for d in near:
        for p in range(AXES):
            line(p, d).start()

    waiting = []

    def pick_rows(p, d):
        if d == 0:
            known, rows_of = facts[...], normed[:, cuts[p] : cuts[p + 1]]
        else:
            known = factg[p * (SIDE - 1) + d - 1]
            rows_of = gath[d - 1, :, cuts[p] : cuts[p + 1]]
        named = jnp.zeros(targets[p].shape, jnp.float32)
        share = jnp.zeros(targets[p].shape, jnp.float32)
        for j in range(choices):
            hit = known[j : j + 1, :] == targets[p]
            named = jnp.where(hit, 1.0, named)
            share = jnp.where(hit, known[choices + j : choices + j + 1, :], share)
        rank = ranks(named)
        ranked[p * SIDE + d] = rank
        shared[p * SIDE + d] = share
        for h in range(0, LINE, CHUNK):
            group = jnp.broadcast_to(rank[h : h + CHUNK][:, None, :], place.shape)
            pick = jnp.where(group == place, 1.0, 0.0).reshape(ROWS, tokens).astype(jnp.bfloat16)
            send[pl.ds((d * LINE + h) * GROUP, ROWS), cuts[p] : cuts[p + 1]] = jnp.dot(
                pick, rows_of, preferred_element_type=jnp.float32
            ).astype(jnp.bfloat16)
            for copy in waiting:
                copy.start()
            waiting[:] = [dispatch(p, d, i) for i in range(h, h + CHUNK)]

    for p in range(AXES):
        pick_rows(p, 0)
    with jax.named_scope("listwait"):
        for copy in listings:
            copy.wait()
    for d in near:
        for p in range(AXES):
            with jax.named_scope("linewait"):
                line(p, d).wait_recv()
            relay(p, d).start()
    for d in near:
        for p in range(AXES):
            pick_rows(p, d)
    for copy in waiting:
        copy.start()
    waiting.clear()
    reach = taps.shape[0] - 1
    for copy in mix_in[:2]:
        copy.wait()
    block = 128

    @pl.loop(0, positions // block)
    def _(b):
        rows = pl.ds(pl.multiple_of(b * block, block), block)
        prod[pl.ds(pl.multiple_of(8 + b * block, 8), block), :] = (
            (gi[rows, :].astype(jnp.float32) * ci[rows, :].astype(jnp.float32))
            .astype(jnp.bfloat16)
            .astype(jnp.float32)
        )

    for copy in mix_in[2:]:
        copy.wait()
    with jax.named_scope('halo_wait'):
        halo_copy.wait()
    prod[0:8, :] = jnp.where(here == 0, 0.0, halo[8:16, :].astype(jnp.float32))

    @pl.loop(0, positions // block)
    def _(b):
        rows = pl.ds(pl.multiple_of(b * block, block), block)
        window = prod[pl.ds(pl.multiple_of(b * block, 8), block + 8), :]
        convolved = jnp.zeros((block, window.shape[1]), jnp.float32)
        for j in range(reach + 1):
            start = 8 - reach + j
            convolved = convolved + taps[j : j + 1, :] * window[start : start + block]
        gated = (go[rows, :].astype(jnp.float32) * convolved).astype(jnp.bfloat16)
        mixed[rows, :] = jnp.dot(
            gated, wmix[...], preferred_element_type=jnp.float32
        ).astype(jnp.bfloat16)

    for p in range(AXES):
        with jax.named_scope("relaywait"):
            for d in near:
                relay(p, d).wait_recv()
        pick_rows(p, 2)
    for copy in waiting:
        copy.start()

    @pl.loop(0, AXES * SIDE)
    def _(n):
        rank = ranked[n]
        share = shared[n]
        for h in range(0, LINE, CHUNK):
            mine = jnp.broadcast_to(rank[h : h + CHUNK][:, None, :], place.shape) == place
            mine = jnp.where(
                mine, jnp.broadcast_to(share[h : h + CHUNK][:, None, :], place.shape), 0.0
            )
            comb[n, :, h * GROUP : h * GROUP + ROWS] = mine.reshape(ROWS, tokens).T.astype(
                jnp.bfloat16
            )

    with jax.named_scope('expw_wait'):
        for copy in experts_in:
            copy.wait()

    @pl.loop(0, TILES)
    def _(c):
        for n in range(TILES):

            @pl.when(c == n)
            def _():
                with jax.named_scope('dwait'):
                    all_rows(recv, drecv.at[n], TILE).wait()

        rows = pl.ds(pl.multiple_of(c * TILE * GROUP, TILE * GROUP), TILE * GROUP)
        block_rows = recv[rows, :]
        hidden = []
        width = 256
        for n in range(0, wg.shape[1], width):
            gate_pre = jnp.dot(
                block_rows, wg[:, n : n + width], preferred_element_type=jnp.float32
            )
            up_pre = jnp.dot(
                block_rows, wu[:, n : n + width], preferred_element_type=jnp.float32
            )
            gate_pre = jnp.minimum(gate_pre, clamp_limit)
            up_pre = jnp.clip(up_pre, -clamp_limit, clamp_limit)
            hidden.append(
                ((up_pre + 1.0) * (gate_pre * jax.nn.sigmoid(alpha_gate * gate_pre))).astype(
                    jnp.bfloat16
                )
            )
        hidden = jnp.concatenate(hidden, axis=1)
        for n in range(0, wd.shape[1], width):
            recv[rows, n : n + width] = jnp.dot(
                hidden, wd[:, n : n + width], preferred_element_type=jnp.float32
            ).astype(jnp.bfloat16)
        for n in range(TILES):

            @pl.when(c == n)
            def _():
                for slot in range(n * TILE, (n + 1) * TILE):
                    for p in range(AXES):
                        if ORDER[slot][p]:
                            giveback(p, slot).start()

    for slot in range(PEERS):
        for p in range(AXES):
            if not ORDER[slot][p]:
                giveback(p, slot).start()

    def added(p, d):
        with jax.named_scope("rwait"):
            part_rows = ret.at[pl.ds(0, LINE * cap), columns(p)]
            pltpu.make_async_copy(part_rows, part_rows, rrecv.at[p * SIDE + d]).wait()
        rows = ret[pl.ds(d * LINE * GROUP, LINE * GROUP), cuts[p] : cuts[p + 1]]
        used = lax.broadcasted_iota(jnp.int32, rows.shape, 0) % GROUP < cap
        rows = jnp.where(used, rows.astype(jnp.float32), 0.0).astype(jnp.bfloat16)
        return jnp.dot(comb[p * SIDE + d], rows, preferred_element_type=jnp.float32)

    for d in BLOCKS:
        for p in range(AXES):
            part[d - 1, :, cuts[p] : cuts[p + 1]] = added(p, d).astype(jnp.bfloat16)
            partial(p, d).start()
    for p in range(AXES):
        acc[:, cuts[p] : cuts[p + 1]] = added(p, 0)
    for p in range(AXES):
        total = acc[:, cuts[p] : cuts[p + 1]]
        for d in BLOCKS:
            with jax.named_scope("bwait"):
                partial(p, d).wait_recv()
            total = total + back[d - 1, :, cuts[p] : cuts[p + 1]].astype(jnp.float32)
        moe[:, cuts[p] : cuts[p + 1]] = total.astype(jnp.bfloat16)
    with jax.named_scope('endwait'):
        all_rows(send, dsend, SIDE * (LINE - 1)).wait()
        pltpu.make_async_copy(gath, gath, gsend).wait()
        all_rows(recv, rsend, SIDE * (LINE - 1)).wait()
        pltpu.make_async_copy(part, part, bsend).wait()


def flush(parts, mixed, moe, mixed_out, moe_out, sem):
    rows = mixed.shape[0] // parts
    copies = [
        pltpu.make_async_copy(
            mixed.at[pl.ds(i * rows, rows)], mixed_out.at[pl.ds(i * rows, rows)], sem.at[i]
        )
        for i in range(parts)
    ]
    copies.append(pltpu.make_async_copy(moe, moe_out, sem.at[parts]))
    for copy in copies:
        copy.start()
    for copy in copies:
        copy.wait()


def shards(
    gate_outer,
    gate_inner,
    conv_input,
    conv_taps,
    mixer_out_weight,
    moe_tokens,
    norm_gain,
    expert_ids,
    route_weight,
    expert_gate,
    expert_up,
    expert_down,
):
    positions, channels = gate_inner.shape
    tokens, width = moe_tokens.shape
    hidden = expert_gate.shape[2]
    choices = expert_ids.shape[1]
    cap = 3 * tokens * choices // (2 * PEERS)
    bf16, f32 = jnp.bfloat16, jnp.float32
    anywhere = pl.BlockSpec(memory_space=pl.ANY)
    slots = (PEERS * GROUP, width)
    mixed, moe = pl.pallas_call(
        functools.partial(kernel, cap),
        out_shape=(
            pltpu.VMEM((positions, width), bf16),
            pltpu.VMEM((tokens, width), bf16),
        ),
        in_specs=[anywhere] * 12,
        out_specs=(pl.BlockSpec(memory_space=pltpu.VMEM), pl.BlockSpec(memory_space=pltpu.VMEM)),
        scratch_shapes=[
            pltpu.VMEM((positions, channels), bf16),
            pltpu.VMEM((positions, channels), bf16),
            pltpu.VMEM((positions, channels), bf16),
            pltpu.VMEM(conv_taps.shape, f32),
            pltpu.VMEM((channels, width), bf16),
            pltpu.VMEM((tokens, width), bf16),
            pltpu.VMEM((1, width), f32),
            pltpu.VMEM((choices, tokens), jnp.int32),
            pltpu.VMEM((choices, tokens), f32),
            pltpu.VMEM((width, hidden), bf16),
            pltpu.VMEM((width, hidden), bf16),
            pltpu.VMEM((hidden, width), bf16),
            pltpu.VMEM(slots, bf16),
            pltpu.VMEM(slots, bf16),
            pltpu.VMEM(slots, bf16),
            pltpu.VMEM((SIDE - 1, tokens, width), bf16),
            pltpu.VMEM((2 * choices, tokens), f32),
            pltpu.VMEM((AXES * (SIDE - 1), 2 * choices, tokens), f32),
            pltpu.VMEM((AXES * SIDE, LINE, tokens), f32),
            pltpu.VMEM((AXES * SIDE, LINE, tokens), f32),
            pltpu.VMEM((SIDE - 1, tokens, width), bf16),
            pltpu.VMEM((SIDE - 1, tokens, width), bf16),
            pltpu.VMEM((AXES * SIDE, tokens, LINE * GROUP), bf16),
            pltpu.VMEM((8 + positions, channels), f32),
            pltpu.VMEM((2, 16, channels), bf16),
            pltpu.VMEM((16, channels), bf16),
            pltpu.VMEM((16, channels), bf16),
            pltpu.VMEM((tokens, width), bf16),
            pltpu.VMEM((tokens, width), f32),
            pltpu.SemaphoreType.DMA((14,)),
            pltpu.SemaphoreType.DMA,
            pltpu.SemaphoreType.DMA((4 * AXES,)),
            pltpu.SemaphoreType.DMA((AXES * (SIDE - 1),)),
            pltpu.SemaphoreType.DMA((AXES * (SIDE - 1),)),
            pltpu.SemaphoreType.DMA,
            pltpu.SemaphoreType.DMA((TILES,)),
            pltpu.SemaphoreType.DMA,
            pltpu.SemaphoreType.DMA((AXES * SIDE,)),
            pltpu.SemaphoreType.DMA,
            pltpu.SemaphoreType.DMA((AXES * (SIDE - 1),)),
            pltpu.SemaphoreType.DMA((2,)),
        ],
        compiler_params=pltpu.CompilerParams(
            collective_id=0, has_side_effects=True, vmem_limit_bytes=56 * 2**20
        ),
        name="layer_step",
    )(
        gate_outer,
        gate_inner,
        conv_input,
        conv_taps,
        mixer_out_weight,
        moe_tokens,
        norm_gain.reshape(1, width),
        expert_ids.T,
        route_weight.T,
        expert_gate.reshape(width, hidden),
        expert_up.reshape(width, hidden),
        expert_down.reshape(hidden, width),
    )
    parts = 4
    return pl.pallas_call(
        functools.partial(flush, parts),
        out_shape=(
            jax.ShapeDtypeStruct(mixed.shape, bf16),
            jax.ShapeDtypeStruct(moe.shape, bf16),
        ),
        in_specs=[pl.BlockSpec(memory_space=pltpu.VMEM)] * 2,
        out_specs=(anywhere, anywhere),
        scratch_shapes=[pltpu.SemaphoreType.DMA((parts + 1,))],
        compiler_params=pltpu.CompilerParams(vmem_limit_bytes=4 * 2**20),
        name="flush",
    )(mixed, moe)


def solution(mesh):
    rows = P(("ep", "tp"), None)
    experts = P(("ep", "tp"), None, None)
    in_specs = (rows, rows, rows, P(), P(), rows, P(), rows, rows, experts, experts, experts)
    return jax.shard_map(
        shards, mesh=mesh, in_specs=in_specs, out_specs=(rows, rows), check_vma=False
    )
```

```python
import functools

import jax
import jax.numpy as jnp
from jax import lax
from jax.experimental import pallas as pl
from jax.experimental.pallas import tpu as pltpu
from jax.sharding import PartitionSpec as P

epsilon = 1e-06
clamp_limit = 7.0
alpha_gate = 1.702
MESH = pl.DeviceIdType.MESH

SIDE = 4
CORES = 2
AXES = 3


def hops(off):
    return sum(min(v, SIDE - v) for v in off[:AXES])


def shuffled(offs, rank_of):
    state = 12345
    keyed = []
    for off in offs:
        state = (state * 1103515245 + 12345) % (1 << 31)
        keyed.append((rank_of(off), state >> 8, off))
    return [k[2] for k in sorted(keyed)]


EVERY = [
    (dz, dy, dx, dk)
    for dz in range(SIDE)
    for dy in range(SIDE)
    for dx in range(SIDE)
    for dk in range(CORES)
]
SELF = (0, 0, 0, 0)
BLOCKS = (2, 1, 3)
ORDER = shuffled(EVERY, lambda off: (off == SELF, 2 in off[:AXES]))
PEERS = len(ORDER)
SLOT = {off: i for i, off in enumerate(ORDER)}
FAR = shuffled(EVERY[1:], lambda off: -hops(off))
PLANE = [shuffled([o for o in EVERY[1:] if o[a] == 0], lambda off: -hops(off)) + [SELF] for a in range(AXES)]
GROUP = 8
CHUNK = 16
TILE = 16
TILES = PEERS // TILE
ROWS = CHUNK * GROUP
LINE = PEERS // SIDE


def kernel(
    cap,
    go_hbm,
    gi_hbm,
    ci_hbm,
    taps_hbm,
    wmix_hbm,
    tok_hbm,
    gain_hbm,
    ids_hbm,
    rw_hbm,
    wg_hbm,
    wu_hbm,
    wd_hbm,
    mixed,
    moe,
    go,
    gi,
    ci,
    taps,
    wmix,
    tok,
    gain,
    ids,
    rw,
    wg,
    wu,
    wd,
    send,
    recv,
    ret,
    gath,
    facts,
    factg,
    ranked,
    shared,
    part,
    back,
    comb,
    prod,
    tails,
    tail,
    halo,
    normed,
    acc,
    lsem,
    gsend,
    grecv,
    isend,
    irecv,
    dsend,
    drecv,
    rsend,
    rrecv,
    bsend,
    brecv,
    hsem,
):
    ep = lax.axis_index("ep")
    tp = lax.axis_index("tp")
    z = ep // (SIDE * CORES)
    y = (ep // CORES) % SIDE
    k = ep % CORES
    x = tp

    def local(i, src, dst):
        copy = pltpu.make_async_copy(src, dst, lsem.at[i])
        copy.start()
        return copy

    positions = gi.shape[0]
    last = pl.ds(positions - 16, 16)
    small = [
        local(0, tok_hbm, tok),
        local(1, ids_hbm, ids),
        local(2, rw_hbm, rw),
        local(3, gain_hbm, gain),
        local(4, gi_hbm.at[last], tails.at[0]),
        local(13, ci_hbm.at[last], tails.at[1]),
    ]

    zs = [(z + d) % SIDE * (SIDE * CORES) for d in range(SIDE)]
    zn = [(z + SIDE - d) % SIDE * (SIDE * CORES) for d in range(SIDE)]
    ys = [(y + d) % SIDE * CORES for d in range(SIDE)]
    yn = [(y + SIDE - d) % SIDE * CORES for d in range(SIDE)]
    xs = [(x + d) % SIDE for d in range(SIDE)]
    xn = [(x + SIDE - d) % SIDE for d in range(SIDE)]
    ks = [(k + d) % CORES for d in range(CORES)]

    def ahead(off):
        dz, dy, dx, dk = off
        return (zs[dz] + ys[dy] + ks[dk], xs[dx])

    def behind(off):
        dz, dy, dx, dk = off
        return (zn[dz] + yn[dy] + ks[dk], xn[dx])

    barrier = pltpu.get_barrier_semaphore()
    for off in FAR:
        pl.semaphore_signal(barrier, inc=1, device_id=ahead(off), device_id_type=MESH)

    mix_in = [
        local(5, gi_hbm, gi),
        local(6, ci_hbm, ci),
        local(7, go_hbm, go),
        local(8, taps_hbm, taps),
        local(9, wmix_hbm, wmix),
    ]
    experts_in = [
        local(10, wg_hbm, wg),
        local(11, wu_hbm, wu),
        local(12, wd_hbm, wd),
    ]

    for copy in small:
        copy.wait()
    wide = tok[...].astype(jnp.float32)
    mean = jnp.mean(wide * wide, axis=-1, keepdims=True)
    normed[...] = (wide * lax.rsqrt(mean + epsilon) * gain[...]).astype(jnp.bfloat16)

    tail[...] = (tails[0].astype(jnp.float32) * tails[1].astype(jnp.float32)).astype(jnp.bfloat16)
    here = ep * SIDE + tp
    after = (here + 1) % PEERS
    halo_copy = pltpu.make_async_remote_copy(
        tail.at[pl.ds(8, 8)],
        halo.at[pl.ds(8, 8)],
        hsem.at[0],
        hsem.at[1],
        device_id=(after // SIDE, after % SIDE),
        device_id_type=MESH,
    )

    tokens = tok.shape[0]
    width = tok.shape[1]
    sublane = lax.broadcasted_iota(jnp.int32, (GROUP, tokens), 0)
    earlier = (
        lax.broadcasted_iota(jnp.int32, (tokens, tokens), 0)
        < lax.broadcasted_iota(jnp.int32, (tokens, tokens), 1)
    ).astype(jnp.bfloat16)
    place = lax.broadcasted_iota(jnp.int32, (CHUNK, GROUP, tokens), 1).astype(jnp.float32)

    def experts_at(offs):
        parts = []
        for i in range(0, len(offs), GROUP):
            codes = [dz * 32 + dy * 8 + dk * 4 + dx for dz, dy, dx, dk in offs[i : i + GROUP]]
            part = jnp.full((GROUP, tokens), codes[0], jnp.int32)
            for j in range(1, GROUP):
                part = jnp.where(sublane == j, codes[j], part)
            parts.append(part)
        off = jnp.concatenate(parts, axis=0)
        oz, oy, ok, ox = off // 32, (off // 8) % SIDE, (off // 4) % CORES, off % SIDE
        return (z + oz) % SIDE * 32 + (y + oy) % SIDE * 8 + (k + ok) % CORES * 4 + (x + ox) % SIDE

    def ranks(named):
        rank = jnp.dot(named.astype(jnp.bfloat16), earlier, preferred_element_type=jnp.float32)
        return jnp.where(named > 0.5, rank, 99.0)

    lanes = width // 128
    cuts = [lanes // AXES * p * 128 for p in range(AXES)] + [width]

    def columns(p):
        return pl.ds(cuts[p], cuts[p + 1] - cuts[p])

    def along(p, d):
        return tuple(d if a == p else 0 for a in range(AXES)) + (0,)

    def line(p, d):
        return pltpu.make_async_remote_copy(
            normed.at[:, columns(p)],
            gath.at[d - 1, :, columns(p)],
            gsend,
            grecv.at[p * 4 + d - 1],
            device_id=ahead(along(p, d)),
            device_id_type=MESH,
        )

    def relay(p, d):
        rows = pl.ds(0 if d == 1 else tokens // 2, tokens // 2)
        return pltpu.make_async_remote_copy(
            gath.at[d - 1, rows, columns(p)],
            gath.at[1, rows, columns(p)],
            gsend,
            grecv.at[p * 4 + (1 if d == 1 else 3)],
            device_id=ahead(along(p, d)),
            device_id_type=MESH,
        )

    def listing(p, d):
        n = p * (SIDE - 1) + d - 1
        return pltpu.make_async_remote_copy(
            facts,
            factg.at[n],
            isend.at[n],
            irecv.at[n],
            device_id=ahead(along(p, d)),
            device_id_type=MESH,
        )

    def dispatch(p, d, i):
        off = PLANE[p][i]
        slot = SLOT[tuple(d if a == p else off[a] for a in range(AXES)) + off[AXES:]]
        source = send.at[pl.ds((d * LINE + i) * GROUP, cap), columns(p)]
        target = recv.at[pl.ds(slot * GROUP, cap), columns(p)]
        if off == SELF:
            return pltpu.make_async_copy(source, target, drecv.at[slot // TILE])
        return pltpu.make_async_remote_copy(
            source,
            target,
            dsend,
            drecv.at[slot // TILE],
            device_id=ahead(off),
            device_id_type=MESH,
        )

    def giveback(p, slot):
        off = ORDER[slot]
        d = off[p]
        flat = tuple(0 if a == p else off[a] for a in range(AXES)) + off[AXES:]
        group = d * LINE + PLANE[p].index(flat)
        source = recv.at[pl.ds(slot * GROUP, cap), columns(p)]
        target = ret.at[pl.ds(group * GROUP, cap), columns(p)]
        if flat == SELF:
            return pltpu.make_async_copy(source, target, rrecv.at[p * SIDE + d])
        return pltpu.make_async_remote_copy(
            source,
            target,
            rsend,
            rrecv.at[p * SIDE + d],
            device_id=behind(flat),
            device_id_type=MESH,
        )

    def partial(p, d):
        return pltpu.make_async_remote_copy(
            part.at[d - 1, :, columns(p)],
            back.at[d - 1, :, columns(p)],
            bsend,
            brecv.at[p * (SIDE - 1) + d - 1],
            device_id=behind(along(p, d)),
            device_id_type=MESH,
        )

    def all_rows(ref, sem, count):
        part = ref.at[pl.ds(0, count * GROUP), pl.ds(0, ref.shape[1] * cap // GROUP)]
        return pltpu.make_async_copy(part, part, sem)

    choices = ids.shape[0]
    weights = rw[...]
    facts[0:choices, :] = ids[...].astype(jnp.float32)
    facts[choices:, :] = weights / jnp.sum(weights, axis=0, keepdims=True)
    targets = [experts_at(PLANE[p]).astype(jnp.float32) for p in range(AXES)]
    with jax.named_scope("barrier"):
        pl.semaphore_wait(barrier, PEERS - 1)
    halo_copy.start()
    near = (1, SIDE - 1)
    listings = [listing(p, d) for d in range(1, SIDE) for p in range(AXES)]
    for copy in listings:
        copy.start()
    for d in near:
        for p in range(AXES):
            line(p, d).start()

    waiting = []
    held = []

    def pick_rows(p, d):
        if d == 0:
            known, rows_of = facts[...], normed[:, cuts[p] : cuts[p + 1]]
        else:
            known = factg[p * (SIDE - 1) + d - 1]
            rows_of = gath[d - 1, :, cuts[p] : cuts[p + 1]]
        named = jnp.zeros(targets[p].shape, jnp.float32)
        share = jnp.zeros(targets[p].shape, jnp.float32)
        for j in range(choices):
            hit = known[j : j + 1, :] == targets[p]
            named = jnp.where(hit, 1.0, named)
            share = jnp.where(hit, known[choices + j : choices + j + 1, :], share)
        rank = ranks(named)
        ranked[p * SIDE + d] = rank
        shared[p * SIDE + d] = share
        for h in range(0, LINE, CHUNK):
            group = jnp.broadcast_to(rank[h : h + CHUNK][:, None, :], place.shape)
            pick = jnp.where(group == place, 1.0, 0.0).reshape(ROWS, tokens).astype(jnp.bfloat16)
            send[pl.ds((d * LINE + h) * GROUP, ROWS), cuts[p] : cuts[p + 1]] = jnp.dot(
                pick, rows_of, preferred_element_type=jnp.float32
            ).astype(jnp.bfloat16)
            for copy in waiting:
                copy.start()
            waiting.clear()
            for i in range(h, h + CHUNK):
                long_way = d in near and 2 in PLANE[p][i][:AXES]
                (held if long_way else waiting).append(dispatch(p, d, i))

    for p in range(AXES):
        pick_rows(p, 0)
    with jax.named_scope("listwait"):
        for copy in listings:
            copy.wait()
    for d in near:
        for p in range(AXES):
            with jax.named_scope("linewait"):
                line(p, d).wait_recv()
            relay(p, d).start()
    for d in near:
        for p in range(AXES):
            pick_rows(p, d)
    for copy in waiting + held:
        copy.start()
    waiting.clear()
    reach = taps.shape[0] - 1
    for copy in mix_in[:2]:
        copy.wait()
    block = 128

    @pl.loop(0, positions // block)
    def _(b):
        rows = pl.ds(pl.multiple_of(b * block, block), block)
        prod[pl.ds(pl.multiple_of(8 + b * block, 8), block), :] = (
            (gi[rows, :].astype(jnp.float32) * ci[rows, :].astype(jnp.float32))
            .astype(jnp.bfloat16)
            .astype(jnp.float32)
        )

    for copy in mix_in[2:]:
        copy.wait()
    with jax.named_scope('halo_wait'):
        halo_copy.wait()
    prod[0:8, :] = jnp.where(here == 0, 0.0, halo[8:16, :].astype(jnp.float32))

    @pl.loop(0, positions // block)
    def _(b):
        rows = pl.ds(pl.multiple_of(b * block, block), block)
        window = prod[pl.ds(pl.multiple_of(b * block, 8), block + 8), :]
        convolved = jnp.zeros((block, window.shape[1]), jnp.float32)
        for j in range(reach + 1):
            start = 8 - reach + j
            convolved = convolved + taps[j : j + 1, :] * window[start : start + block]
        gated = (go[rows, :].astype(jnp.float32) * convolved).astype(jnp.bfloat16)
        mixed[rows, :] = jnp.dot(
            gated, wmix[...], preferred_element_type=jnp.float32
        ).astype(jnp.bfloat16)

    for p in range(AXES):
        with jax.named_scope("relaywait"):
            for d in near:
                relay(p, d).wait_recv()
        pick_rows(p, 2)
    for copy in waiting:
        copy.start()

    @pl.loop(0, AXES * SIDE)
    def _(n):
        rank = ranked[n]
        share = shared[n]
        for h in range(0, LINE, CHUNK):
            mine = jnp.broadcast_to(rank[h : h + CHUNK][:, None, :], place.shape) == place
            mine = jnp.where(
                mine, jnp.broadcast_to(share[h : h + CHUNK][:, None, :], place.shape), 0.0
            )
            comb[n, :, h * GROUP : h * GROUP + ROWS] = mine.reshape(ROWS, tokens).T.astype(
                jnp.bfloat16
            )

    with jax.named_scope('expw_wait'):
        for copy in experts_in:
            copy.wait()

    @pl.loop(0, TILES)
    def _(c):
        for n in range(TILES):

            @pl.when(c == n)
            def _():
                with jax.named_scope('dwait'):
                    all_rows(recv, drecv.at[n], TILE).wait()

        rows = pl.ds(pl.multiple_of(c * TILE * GROUP, TILE * GROUP), TILE * GROUP)
        block_rows = recv[rows, :]
        hidden = []
        width = 256
        for n in range(0, wg.shape[1], width):
            gate_pre = jnp.dot(
                block_rows, wg[:, n : n + width], preferred_element_type=jnp.float32
            )
            up_pre = jnp.dot(
                block_rows, wu[:, n : n + width], preferred_element_type=jnp.float32
            )
            gate_pre = jnp.minimum(gate_pre, clamp_limit)
            up_pre = jnp.clip(up_pre, -clamp_limit, clamp_limit)
            hidden.append(
                ((up_pre + 1.0) * (gate_pre * jax.nn.sigmoid(alpha_gate * gate_pre))).astype(
                    jnp.bfloat16
                )
            )
        hidden = jnp.concatenate(hidden, axis=1)
        for n in range(0, wd.shape[1], width):
            recv[rows, n : n + width] = jnp.dot(
                hidden, wd[:, n : n + width], preferred_element_type=jnp.float32
            ).astype(jnp.bfloat16)
        for n in range(TILES):

            @pl.when(c == n)
            def _():
                for slot in range(n * TILE, (n + 1) * TILE):
                    for p in range(AXES):
                        if ORDER[slot][p]:
                            giveback(p, slot).start()

    for slot in range(PEERS):
        for p in range(AXES):
            if not ORDER[slot][p]:
                giveback(p, slot).start()

    def added(p, d):
        with jax.named_scope("rwait"):
            part_rows = ret.at[pl.ds(0, LINE * cap), columns(p)]
            pltpu.make_async_copy(part_rows, part_rows, rrecv.at[p * SIDE + d]).wait()
        rows = ret[pl.ds(d * LINE * GROUP, LINE * GROUP), cuts[p] : cuts[p + 1]]
        used = lax.broadcasted_iota(jnp.int32, rows.shape, 0) % GROUP < cap
        rows = jnp.where(used, rows.astype(jnp.float32), 0.0).astype(jnp.bfloat16)
        return jnp.dot(comb[p * SIDE + d], rows, preferred_element_type=jnp.float32)

    for d in BLOCKS:
        for p in range(AXES):
            part[d - 1, :, cuts[p] : cuts[p + 1]] = added(p, d).astype(jnp.bfloat16)
            partial(p, d).start()
    for p in range(AXES):
        acc[:, cuts[p] : cuts[p + 1]] = added(p, 0)
    for p in range(AXES):
        total = acc[:, cuts[p] : cuts[p + 1]]
        for d in BLOCKS:
            with jax.named_scope("bwait"):
                partial(p, d).wait_recv()
            total = total + back[d - 1, :, cuts[p] : cuts[p + 1]].astype(jnp.float32)
        moe[:, cuts[p] : cuts[p + 1]] = total.astype(jnp.bfloat16)
    with jax.named_scope('endwait'):
        all_rows(send, dsend, SIDE * (LINE - 1)).wait()
        pltpu.make_async_copy(gath, gath, gsend).wait()
        all_rows(recv, rsend, SIDE * (LINE - 1)).wait()
        pltpu.make_async_copy(part, part, bsend).wait()


def flush(parts, mixed, moe, mixed_out, moe_out, sem):
    rows = mixed.shape[0] // parts
    copies = [
        pltpu.make_async_copy(
            mixed.at[pl.ds(i * rows, rows)], mixed_out.at[pl.ds(i * rows, rows)], sem.at[i]
        )
        for i in range(parts)
    ]
    copies.append(pltpu.make_async_copy(moe, moe_out, sem.at[parts]))
    for copy in copies:
        copy.start()
    for copy in copies:
        copy.wait()


def shards(
    gate_outer,
    gate_inner,
    conv_input,
    conv_taps,
    mixer_out_weight,
    moe_tokens,
    norm_gain,
    expert_ids,
    route_weight,
    expert_gate,
    expert_up,
    expert_down,
):
    positions, channels = gate_inner.shape
    tokens, width = moe_tokens.shape
    hidden = expert_gate.shape[2]
    choices = expert_ids.shape[1]
    cap = 3 * tokens * choices // (2 * PEERS)
    bf16, f32 = jnp.bfloat16, jnp.float32
    anywhere = pl.BlockSpec(memory_space=pl.ANY)
    slots = (PEERS * GROUP, width)
    mixed, moe = pl.pallas_call(
        functools.partial(kernel, cap),
        out_shape=(
            pltpu.VMEM((positions, width), bf16),
            pltpu.VMEM((tokens, width), bf16),
        ),
        in_specs=[anywhere] * 12,
        out_specs=(pl.BlockSpec(memory_space=pltpu.VMEM), pl.BlockSpec(memory_space=pltpu.VMEM)),
        scratch_shapes=[
            pltpu.VMEM((positions, channels), bf16),
            pltpu.VMEM((positions, channels), bf16),
            pltpu.VMEM((positions, channels), bf16),
            pltpu.VMEM(conv_taps.shape, f32),
            pltpu.VMEM((channels, width), bf16),
            pltpu.VMEM((tokens, width), bf16),
            pltpu.VMEM((1, width), f32),
            pltpu.VMEM((choices, tokens), jnp.int32),
            pltpu.VMEM((choices, tokens), f32),
            pltpu.VMEM((width, hidden), bf16),
            pltpu.VMEM((width, hidden), bf16),
            pltpu.VMEM((hidden, width), bf16),
            pltpu.VMEM(slots, bf16),
            pltpu.VMEM(slots, bf16),
            pltpu.VMEM(slots, bf16),
            pltpu.VMEM((SIDE - 1, tokens, width), bf16),
            pltpu.VMEM((2 * choices, tokens), f32),
            pltpu.VMEM((AXES * (SIDE - 1), 2 * choices, tokens), f32),
            pltpu.VMEM((AXES * SIDE, LINE, tokens), f32),
            pltpu.VMEM((AXES * SIDE, LINE, tokens), f32),
            pltpu.VMEM((SIDE - 1, tokens, width), bf16),
            pltpu.VMEM((SIDE - 1, tokens, width), bf16),
            pltpu.VMEM((AXES * SIDE, tokens, LINE * GROUP), bf16),
            pltpu.VMEM((8 + positions, channels), f32),
            pltpu.VMEM((2, 16, channels), bf16),
            pltpu.VMEM((16, channels), bf16),
            pltpu.VMEM((16, channels), bf16),
            pltpu.VMEM((tokens, width), bf16),
            pltpu.VMEM((tokens, width), f32),
            pltpu.SemaphoreType.DMA((14,)),
            pltpu.SemaphoreType.DMA,
            pltpu.SemaphoreType.DMA((4 * AXES,)),
            pltpu.SemaphoreType.DMA((AXES * (SIDE - 1),)),
            pltpu.SemaphoreType.DMA((AXES * (SIDE - 1),)),
            pltpu.SemaphoreType.DMA,
            pltpu.SemaphoreType.DMA((TILES,)),
            pltpu.SemaphoreType.DMA,
            pltpu.SemaphoreType.DMA((AXES * SIDE,)),
            pltpu.SemaphoreType.DMA,
            pltpu.SemaphoreType.DMA((AXES * (SIDE - 1),)),
            pltpu.SemaphoreType.DMA((2,)),
        ],
        compiler_params=pltpu.CompilerParams(
            collective_id=0, has_side_effects=True, vmem_limit_bytes=56 * 2**20
        ),
        name="layer_step",
    )(
        gate_outer,
        gate_inner,
        conv_input,
        conv_taps,
        mixer_out_weight,
        moe_tokens,
        norm_gain.reshape(1, width),
        expert_ids.T,
        route_weight.T,
        expert_gate.reshape(width, hidden),
        expert_up.reshape(width, hidden),
        expert_down.reshape(hidden, width),
    )
    parts = 4
    return pl.pallas_call(
        functools.partial(flush, parts),
        out_shape=(
            jax.ShapeDtypeStruct(mixed.shape, bf16),
            jax.ShapeDtypeStruct(moe.shape, bf16),
        ),
        in_specs=[pl.BlockSpec(memory_space=pltpu.VMEM)] * 2,
        out_specs=(anywhere, anywhere),
        scratch_shapes=[pltpu.SemaphoreType.DMA((parts + 1,))],
        compiler_params=pltpu.CompilerParams(vmem_limit_bytes=4 * 2**20),
        name="flush",
    )(mixed, moe)


def solution(mesh):
    rows = P(("ep", "tp"), None)
    experts = P(("ep", "tp"), None, None)
    in_specs = (rows, rows, rows, P(), P(), rows, P(), rows, rows, experts, experts, experts)
    return jax.shard_map(
        shards, mesh=mesh, in_specs=in_specs, out_specs=(rows, rows), check_vma=False
    )
```

```python
import functools

import jax
import jax.numpy as jnp
from jax import lax
from jax.experimental import pallas as pl
from jax.experimental.pallas import tpu as pltpu
from jax.sharding import PartitionSpec as P

epsilon = 1e-06
clamp_limit = 7.0
alpha_gate = 1.702
MESH = pl.DeviceIdType.MESH

SIDE = 4
CORES = 2
AXES = 3


def hops(off):
    return sum(min(v, SIDE - v) for v in off[:AXES])


def shuffled(offs, rank_of):
    state = 777
    keyed = []
    for off in offs:
        state = (state * 1103515245 + 12345) % (1 << 31)
        keyed.append((rank_of(off), state >> 8, off))
    return [k[2] for k in sorted(keyed)]


EVERY = [
    (dz, dy, dx, dk)
    for dz in range(SIDE)
    for dy in range(SIDE)
    for dx in range(SIDE)
    for dk in range(CORES)
]
SELF = (0, 0, 0, 0)
BLOCKS = (2, 1, 3)
ORDER = shuffled(EVERY, lambda off: (off == SELF, 2 in off[:AXES]))
PEERS = len(ORDER)
SLOT = {off: i for i, off in enumerate(ORDER)}
FAR = shuffled(EVERY[1:], lambda off: -hops(off))
PLANE = [shuffled([o for o in EVERY[1:] if o[a] == 0], lambda off: -hops(off)) + [SELF] for a in range(AXES)]
GROUP = 8
CHUNK = 16
TILE = 16
TILES = PEERS // TILE
ROWS = CHUNK * GROUP
LINE = PEERS // SIDE


def kernel(
    cap,
    go_hbm,
    gi_hbm,
    ci_hbm,
    taps_hbm,
    wmix_hbm,
    tok_hbm,
    gain_hbm,
    ids_hbm,
    rw_hbm,
    wg_hbm,
    wu_hbm,
    wd_hbm,
    mixed,
    moe,
    go,
    gi,
    ci,
    taps,
    wmix,
    tok,
    gain,
    ids,
    rw,
    wg,
    wu,
    wd,
    send,
    recv,
    ret,
    gath,
    facts,
    factg,
    ranked,
    shared,
    part,
    back,
    comb,
    prod,
    tails,
    tail,
    halo,
    normed,
    acc,
    lsem,
    gsend,
    grecv,
    isend,
    irecv,
    dsend,
    drecv,
    rsend,
    rrecv,
    bsend,
    brecv,
    hsem,
):
    ep = lax.axis_index("ep")
    tp = lax.axis_index("tp")
    z = ep // (SIDE * CORES)
    y = (ep // CORES) % SIDE
    k = ep % CORES
    x = tp

    def local(i, src, dst):
        copy = pltpu.make_async_copy(src, dst, lsem.at[i])
        copy.start()
        return copy

    positions = gi.shape[0]
    last = pl.ds(positions - 16, 16)
    small = [
        local(0, tok_hbm, tok),
        local(1, ids_hbm, ids),
        local(2, rw_hbm, rw),
        local(3, gain_hbm, gain),
        local(4, gi_hbm.at[last], tails.at[0]),
        local(13, ci_hbm.at[last], tails.at[1]),
    ]

    zs = [(z + d) % SIDE * (SIDE * CORES) for d in range(SIDE)]
    zn = [(z + SIDE - d) % SIDE * (SIDE * CORES) for d in range(SIDE)]
    ys = [(y + d) % SIDE * CORES for d in range(SIDE)]
    yn = [(y + SIDE - d) % SIDE * CORES for d in range(SIDE)]
    xs = [(x + d) % SIDE for d in range(SIDE)]
    xn = [(x + SIDE - d) % SIDE for d in range(SIDE)]
    ks = [(k + d) % CORES for d in range(CORES)]

    def ahead(off):
        dz, dy, dx, dk = off
        return (zs[dz] + ys[dy] + ks[dk], xs[dx])

    def behind(off):
        dz, dy, dx, dk = off
        return (zn[dz] + yn[dy] + ks[dk], xn[dx])

    barrier = pltpu.get_barrier_semaphore()
    for off in FAR:
        pl.semaphore_signal(barrier, inc=1, device_id=ahead(off), device_id_type=MESH)

    mix_in = [
        local(5, gi_hbm, gi),
        local(6, ci_hbm, ci),
        local(7, go_hbm, go),
        local(8, taps_hbm, taps),
        local(9, wmix_hbm, wmix),
    ]
    experts_in = [
        local(10, wg_hbm, wg),
        local(11, wu_hbm, wu),
        local(12, wd_hbm, wd),
    ]

    for copy in small:
        copy.wait()
    wide = tok[...].astype(jnp.float32)
    mean = jnp.mean(wide * wide, axis=-1, keepdims=True)
    normed[...] = (wide * lax.rsqrt(mean + epsilon) * gain[...]).astype(jnp.bfloat16)

    tail[...] = (tails[0].astype(jnp.float32) * tails[1].astype(jnp.float32)).astype(jnp.bfloat16)
    here = ep * SIDE + tp
    after = (here + 1) % PEERS
    halo_copy = pltpu.make_async_remote_copy(
        tail.at[pl.ds(8, 8)],
        halo.at[pl.ds(8, 8)],
        hsem.at[0],
        hsem.at[1],
        device_id=(after // SIDE, after % SIDE),
        device_id_type=MESH,
    )

    tokens = tok.shape[0]
    width = tok.shape[1]
    sublane = lax.broadcasted_iota(jnp.int32, (GROUP, tokens), 0)
    earlier = (
        lax.broadcasted_iota(jnp.int32, (tokens, tokens), 0)
        < lax.broadcasted_iota(jnp.int32, (tokens, tokens), 1)
    ).astype(jnp.bfloat16)
    place = lax.broadcasted_iota(jnp.int32, (CHUNK, GROUP, tokens), 1).astype(jnp.float32)

    def experts_at(offs):
        parts = []
        for i in range(0, len(offs), GROUP):
            codes = [dz * 32 + dy * 8 + dk * 4 + dx for dz, dy, dx, dk in offs[i : i + GROUP]]
            part = jnp.full((GROUP, tokens), codes[0], jnp.int32)
            for j in range(1, GROUP):
                part = jnp.where(sublane == j, codes[j], part)
            parts.append(part)
        off = jnp.concatenate(parts, axis=0)
        oz, oy, ok, ox = off // 32, (off // 8) % SIDE, (off // 4) % CORES, off % SIDE
        return (z + oz) % SIDE * 32 + (y + oy) % SIDE * 8 + (k + ok) % CORES * 4 + (x + ox) % SIDE

    def ranks(named):
        rank = jnp.dot(named.astype(jnp.bfloat16), earlier, preferred_element_type=jnp.float32)
        return jnp.where(named > 0.5, rank, 99.0)

    lanes = width // 128
    cuts = [lanes // AXES * p * 128 for p in range(AXES)] + [width]

    def columns(p):
        return pl.ds(cuts[p], cuts[p + 1] - cuts[p])

    def along(p, d):
        return tuple(d if a == p else 0 for a in range(AXES)) + (0,)

    def line(p, d):
        return pltpu.make_async_remote_copy(
            normed.at[:, columns(p)],
            gath.at[d - 1, :, columns(p)],
            gsend,
            grecv.at[p * 4 + d - 1],
            device_id=ahead(along(p, d)),
            device_id_type=MESH,
        )

    def relay(p, d):
        rows = pl.ds(0 if d == 1 else tokens // 2, tokens // 2)
        return pltpu.make_async_remote_copy(
            gath.at[d - 1, rows, columns(p)],
            gath.at[1, rows, columns(p)],
            gsend,
            grecv.at[p * 4 + (1 if d == 1 else 3)],
            device_id=ahead(along(p, d)),
            device_id_type=MESH,
        )

    def listing(p, d):
        n = p * (SIDE - 1) + d - 1
        return pltpu.make_async_remote_copy(
            facts,
            factg.at[n],
            isend.at[n],
            irecv.at[n],
            device_id=ahead(along(p, d)),
            device_id_type=MESH,
        )

    def dispatch(p, d, i):
        off = PLANE[p][i]
        slot = SLOT[tuple(d if a == p else off[a] for a in range(AXES)) + off[AXES:]]
        source = send.at[pl.ds((d * LINE + i) * GROUP, cap), columns(p)]
        target = recv.at[pl.ds(slot * GROUP, cap), columns(p)]
        if off == SELF:
            return pltpu.make_async_copy(source, target, drecv.at[slot // TILE])
        return pltpu.make_async_remote_copy(
            source,
            target,
            dsend,
            drecv.at[slot // TILE],
            device_id=ahead(off),
            device_id_type=MESH,
        )

    def giveback(p, slot):
        off = ORDER[slot]
        d = off[p]
        flat = tuple(0 if a == p else off[a] for a in range(AXES)) + off[AXES:]
        group = d * LINE + PLANE[p].index(flat)
        source = recv.at[pl.ds(slot * GROUP, cap), columns(p)]
        target = ret.at[pl.ds(group * GROUP, cap), columns(p)]
        if flat == SELF:
            return pltpu.make_async_copy(source, target, rrecv.at[p * SIDE + d])
        return pltpu.make_async_remote_copy(
            source,
            target,
            rsend,
            rrecv.at[p * SIDE + d],
            device_id=behind(flat),
            device_id_type=MESH,
        )

    def partial(p, d):
        return pltpu.make_async_remote_copy(
            part.at[d - 1, :, columns(p)],
            back.at[d - 1, :, columns(p)],
            bsend,
            brecv.at[p * (SIDE - 1) + d - 1],
            device_id=behind(along(p, d)),
            device_id_type=MESH,
        )

    def all_rows(ref, sem, count):
        part = ref.at[pl.ds(0, count * GROUP), pl.ds(0, ref.shape[1] * cap // GROUP)]
        return pltpu.make_async_copy(part, part, sem)

    choices = ids.shape[0]
    weights = rw[...]
    facts[0:choices, :] = ids[...].astype(jnp.float32)
    facts[choices:, :] = weights / jnp.sum(weights, axis=0, keepdims=True)
    targets = [experts_at(PLANE[p]).astype(jnp.float32) for p in range(AXES)]
    with jax.named_scope("barrier"):
        pl.semaphore_wait(barrier, PEERS - 1)
    halo_copy.start()
    near = (1, SIDE - 1)
    listings = [listing(p, d) for d in range(1, SIDE) for p in range(AXES)]
    for copy in listings:
        copy.start()
    for d in near:
        for p in range(AXES):
            line(p, d).start()

    waiting = []
    held = []

    def pick_rows(p, d):
        if d == 0:
            known, rows_of = facts[...], normed[:, cuts[p] : cuts[p + 1]]
        else:
            known = factg[p * (SIDE - 1) + d - 1]
            rows_of = gath[d - 1, :, cuts[p] : cuts[p + 1]]
        named = jnp.zeros(targets[p].shape, jnp.float32)
        share = jnp.zeros(targets[p].shape, jnp.float32)
        for j in range(choices):
            hit = known[j : j + 1, :] == targets[p]
            named = jnp.where(hit, 1.0, named)
            share = jnp.where(hit, known[choices + j : choices + j + 1, :], share)
        rank = ranks(named)
        ranked[p * SIDE + d] = rank
        shared[p * SIDE + d] = share
        for h in range(0, LINE, CHUNK):
            group = jnp.broadcast_to(rank[h : h + CHUNK][:, None, :], place.shape)
            pick = jnp.where(group == place, 1.0, 0.0).reshape(ROWS, tokens).astype(jnp.bfloat16)
            send[pl.ds((d * LINE + h) * GROUP, ROWS), cuts[p] : cuts[p + 1]] = jnp.dot(
                pick, rows_of, preferred_element_type=jnp.float32
            ).astype(jnp.bfloat16)
            for copy in waiting:
                copy.start()
            waiting.clear()
            for i in range(h, h + CHUNK):
                long_way = d in near and 2 in PLANE[p][i][:AXES]
                (held if long_way else waiting).append(dispatch(p, d, i))

    for p in range(AXES):
        pick_rows(p, 0)
    with jax.named_scope("listwait"):
        for copy in listings:
            copy.wait()
    for d in near:
        for p in range(AXES):
            with jax.named_scope("linewait"):
                line(p, d).wait_recv()
            relay(p, d).start()
    for d in near:
        for p in range(AXES):
            pick_rows(p, d)
    for copy in waiting + held:
        copy.start()
    waiting.clear()
    reach = taps.shape[0] - 1
    for copy in mix_in[:2]:
        copy.wait()
    block = 128

    @pl.loop(0, positions // block)
    def _(b):
        rows = pl.ds(pl.multiple_of(b * block, block), block)
        prod[pl.ds(pl.multiple_of(8 + b * block, 8), block), :] = (
            (gi[rows, :].astype(jnp.float32) * ci[rows, :].astype(jnp.float32))
            .astype(jnp.bfloat16)
            .astype(jnp.float32)
        )

    for copy in mix_in[2:]:
        copy.wait()
    with jax.named_scope('halo_wait'):
        halo_copy.wait()
    prod[0:8, :] = jnp.where(here == 0, 0.0, halo[8:16, :].astype(jnp.float32))

    @pl.loop(0, positions // block)
    def _(b):
        rows = pl.ds(pl.multiple_of(b * block, block), block)
        window = prod[pl.ds(pl.multiple_of(b * block, 8), block + 8), :]
        convolved = jnp.zeros((block, window.shape[1]), jnp.float32)
        for j in range(reach + 1):
            start = 8 - reach + j
            convolved = convolved + taps[j : j + 1, :] * window[start : start + block]
        gated = (go[rows, :].astype(jnp.float32) * convolved).astype(jnp.bfloat16)
        mixed[rows, :] = jnp.dot(
            gated, wmix[...], preferred_element_type=jnp.float32
        ).astype(jnp.bfloat16)

    for p in range(AXES):
        with jax.named_scope("relaywait"):
            for d in near:
                relay(p, d).wait_recv()
        pick_rows(p, 2)
    for copy in waiting:
        copy.start()

    @pl.loop(0, AXES * SIDE)
    def _(n):
        rank = ranked[n]
        share = shared[n]
        for h in range(0, LINE, CHUNK):
            mine = jnp.broadcast_to(rank[h : h + CHUNK][:, None, :], place.shape) == place
            mine = jnp.where(
                mine, jnp.broadcast_to(share[h : h + CHUNK][:, None, :], place.shape), 0.0
            )
            comb[n, :, h * GROUP : h * GROUP + ROWS] = mine.reshape(ROWS, tokens).T.astype(
                jnp.bfloat16
            )

    with jax.named_scope('expw_wait'):
        for copy in experts_in:
            copy.wait()

    @pl.loop(0, TILES)
    def _(c):
        for n in range(TILES):

            @pl.when(c == n)
            def _():
                with jax.named_scope('dwait'):
                    all_rows(recv, drecv.at[n], TILE).wait()

        rows = pl.ds(pl.multiple_of(c * TILE * GROUP, TILE * GROUP), TILE * GROUP)
        block_rows = recv[rows, :]
        hidden = []
        width = 256
        for n in range(0, wg.shape[1], width):
            gate_pre = jnp.dot(
                block_rows, wg[:, n : n + width], preferred_element_type=jnp.float32
            )
            up_pre = jnp.dot(
                block_rows, wu[:, n : n + width], preferred_element_type=jnp.float32
            )
            gate_pre = jnp.minimum(gate_pre, clamp_limit)
            up_pre = jnp.clip(up_pre, -clamp_limit, clamp_limit)
            hidden.append(
                ((up_pre + 1.0) * (gate_pre * jax.nn.sigmoid(alpha_gate * gate_pre))).astype(
                    jnp.bfloat16
                )
            )
        hidden = jnp.concatenate(hidden, axis=1)
        for n in range(0, wd.shape[1], width):
            recv[rows, n : n + width] = jnp.dot(
                hidden, wd[:, n : n + width], preferred_element_type=jnp.float32
            ).astype(jnp.bfloat16)
        for n in range(TILES):

            @pl.when(c == n)
            def _():
                for slot in range(n * TILE, (n + 1) * TILE):
                    for p in range(AXES):
                        if ORDER[slot][p]:
                            giveback(p, slot).start()

    for slot in range(PEERS):
        for p in range(AXES):
            if not ORDER[slot][p]:
                giveback(p, slot).start()

    def added(p, d):
        with jax.named_scope("rwait"):
            part_rows = ret.at[pl.ds(0, LINE * cap), columns(p)]
            pltpu.make_async_copy(part_rows, part_rows, rrecv.at[p * SIDE + d]).wait()
        rows = ret[pl.ds(d * LINE * GROUP, LINE * GROUP), cuts[p] : cuts[p + 1]]
        used = lax.broadcasted_iota(jnp.int32, rows.shape, 0) % GROUP < cap
        rows = jnp.where(used, rows.astype(jnp.float32), 0.0).astype(jnp.bfloat16)
        return jnp.dot(comb[p * SIDE + d], rows, preferred_element_type=jnp.float32)

    for d in BLOCKS:
        for p in range(AXES):
            part[d - 1, :, cuts[p] : cuts[p + 1]] = added(p, d).astype(jnp.bfloat16)
            partial(p, d).start()
    for p in range(AXES):
        acc[:, cuts[p] : cuts[p + 1]] = added(p, 0)
    for p in range(AXES):
        total = acc[:, cuts[p] : cuts[p + 1]]
        for d in BLOCKS:
            with jax.named_scope("bwait"):
                partial(p, d).wait_recv()
            total = total + back[d - 1, :, cuts[p] : cuts[p + 1]].astype(jnp.float32)
        moe[:, cuts[p] : cuts[p + 1]] = total.astype(jnp.bfloat16)
    with jax.named_scope('endwait'):
        all_rows(send, dsend, SIDE * (LINE - 1)).wait()
        pltpu.make_async_copy(gath, gath, gsend).wait()
        all_rows(recv, rsend, SIDE * (LINE - 1)).wait()
        pltpu.make_async_copy(part, part, bsend).wait()


def flush(parts, mixed, moe, mixed_out, moe_out, sem):
    rows = mixed.shape[0] // parts
    copies = [
        pltpu.make_async_copy(
            mixed.at[pl.ds(i * rows, rows)], mixed_out.at[pl.ds(i * rows, rows)], sem.at[i]
        )
        for i in range(parts)
    ]
    copies.append(pltpu.make_async_copy(moe, moe_out, sem.at[parts]))
    for copy in copies:
        copy.start()
    for copy in copies:
        copy.wait()


def shards(
    gate_outer,
    gate_inner,
    conv_input,
    conv_taps,
    mixer_out_weight,
    moe_tokens,
    norm_gain,
    expert_ids,
    route_weight,
    expert_gate,
    expert_up,
    expert_down,
):
    positions, channels = gate_inner.shape
    tokens, width = moe_tokens.shape
    hidden = expert_gate.shape[2]
    choices = expert_ids.shape[1]
    cap = 3 * tokens * choices // (2 * PEERS)
    bf16, f32 = jnp.bfloat16, jnp.float32
    anywhere = pl.BlockSpec(memory_space=pl.ANY)
    slots = (PEERS * GROUP, width)
    mixed, moe = pl.pallas_call(
        functools.partial(kernel, cap),
        out_shape=(
            pltpu.VMEM((positions, width), bf16),
            pltpu.VMEM((tokens, width), bf16),
        ),
        in_specs=[anywhere] * 12,
        out_specs=(pl.BlockSpec(memory_space=pltpu.VMEM), pl.BlockSpec(memory_space=pltpu.VMEM)),
        scratch_shapes=[
            pltpu.VMEM((positions, channels), bf16),
            pltpu.VMEM((positions, channels), bf16),
            pltpu.VMEM((positions, channels), bf16),
            pltpu.VMEM(conv_taps.shape, f32),
            pltpu.VMEM((channels, width), bf16),
            pltpu.VMEM((tokens, width), bf16),
            pltpu.VMEM((1, width), f32),
            pltpu.VMEM((choices, tokens), jnp.int32),
            pltpu.VMEM((choices, tokens), f32),
            pltpu.VMEM((width, hidden), bf16),
            pltpu.VMEM((width, hidden), bf16),
            pltpu.VMEM((hidden, width), bf16),
            pltpu.VMEM(slots, bf16),
            pltpu.VMEM(slots, bf16),
            pltpu.VMEM(slots, bf16),
            pltpu.VMEM((SIDE - 1, tokens, width), bf16),
            pltpu.VMEM((2 * choices, tokens), f32),
            pltpu.VMEM((AXES * (SIDE - 1), 2 * choices, tokens), f32),
            pltpu.VMEM((AXES * SIDE, LINE, tokens), f32),
            pltpu.VMEM((AXES * SIDE, LINE, tokens), f32),
            pltpu.VMEM((SIDE - 1, tokens, width), bf16),
            pltpu.VMEM((SIDE - 1, tokens, width), bf16),
            pltpu.VMEM((AXES * SIDE, tokens, LINE * GROUP), bf16),
            pltpu.VMEM((8 + positions, channels), f32),
            pltpu.VMEM((2, 16, channels), bf16),
            pltpu.VMEM((16, channels), bf16),
            pltpu.VMEM((16, channels), bf16),
            pltpu.VMEM((tokens, width), bf16),
            pltpu.VMEM((tokens, width), f32),
            pltpu.SemaphoreType.DMA((14,)),
            pltpu.SemaphoreType.DMA,
            pltpu.SemaphoreType.DMA((4 * AXES,)),
            pltpu.SemaphoreType.DMA((AXES * (SIDE - 1),)),
            pltpu.SemaphoreType.DMA((AXES * (SIDE - 1),)),
            pltpu.SemaphoreType.DMA,
            pltpu.SemaphoreType.DMA((TILES,)),
            pltpu.SemaphoreType.DMA,
            pltpu.SemaphoreType.DMA((AXES * SIDE,)),
            pltpu.SemaphoreType.DMA,
            pltpu.SemaphoreType.DMA((AXES * (SIDE - 1),)),
            pltpu.SemaphoreType.DMA((2,)),
        ],
        compiler_params=pltpu.CompilerParams(
            collective_id=0, has_side_effects=True, vmem_limit_bytes=56 * 2**20
        ),
        name="layer_step",
    )(
        gate_outer,
        gate_inner,
        conv_input,
        conv_taps,
        mixer_out_weight,
        moe_tokens,
        norm_gain.reshape(1, width),
        expert_ids.T,
        route_weight.T,
        expert_gate.reshape(width, hidden),
        expert_up.reshape(width, hidden),
        expert_down.reshape(hidden, width),
    )
    parts = 4
    return pl.pallas_call(
        functools.partial(flush, parts),
        out_shape=(
            jax.ShapeDtypeStruct(mixed.shape, bf16),
            jax.ShapeDtypeStruct(moe.shape, bf16),
        ),
        in_specs=[pl.BlockSpec(memory_space=pltpu.VMEM)] * 2,
        out_specs=(anywhere, anywhere),
        scratch_shapes=[pltpu.SemaphoreType.DMA((parts + 1,))],
        compiler_params=pltpu.CompilerParams(vmem_limit_bytes=4 * 2**20),
        name="flush",
    )(mixed, moe)


def solution(mesh):
    rows = P(("ep", "tp"), None)
    experts = P(("ep", "tp"), None, None)
    in_specs = (rows, rows, rows, P(), P(), rows, P(), rows, rows, experts, experts, experts)
    return jax.shard_map(
        shards, mesh=mesh, in_specs=in_specs, out_specs=(rows, rows), check_vma=False
    )
```
